128 devices in a mesh: sp: 16 (over z, y), dp: 8 (over x, core).
Axes of the slice: x: 4, y: 4, z: 4, core: 2. Of those that a mesh axis runs over, the one named last changes fastest.
Arguments:
- u_pre: bfloat16 [8, 16384, 2048], P('dp', 'sp'), may hold values from -6 to 6
- v_pre: bfloat16 [8, 16384, 2048], P('dp', 'sp'), may hold values from -6 to 6
- d_out: bfloat16 [8, 16384, 2048], P('dp', 'sp'), may hold values from -6 to 6
- w_mix: bfloat16 [16, 128, 128], replicated, may hold values from -0.5 to 0.5
- mix_bias: float32 [16, 128], replicated, may hold values from 0.1 to 1.9
- norm_gain: float32 [16, 128], replicated, may hold values from 0.1 to 1.9
- norm_shift: float32 [16, 128], replicated, may hold values from -3 to 3
- w_out: bfloat16 [2048, 2048], P('dp'), may hold values from -0.125 to 0.125
Outputs:
- grad_u: bfloat16 [8, 16384, 2048], P('dp', 'sp')
- grad_v: bfloat16 [8, 16384, 2048], P('dp', 'sp')
- grad_w_out: float32 [2048, 2048], P('dp')
- grad_w_mix: float32 [16, 128, 128], replicated
- grad_mix_bias: float32 [16, 128], replicated
- grad_gain: float32 [16, 128], replicated
- grad_shift: float32 [16, 128], replicated
The draws below stay inside these ranges and needn't reach their ends.
All inputs are finite; a program needn't handle non-finite values.
Results may differ from the reference program's by a relative error of at most 0.012.
Values may be sent and summed in bfloat16 or wider, within the bound.
A program may use at most 192 MiB of HBM per device.

```python
import jax
import jax.numpy as jnp
from jax import lax

D = 2048
GROUPS = 16
CHANS = 128
BLOCK = 128
SGU_W = 2048
SEQLEN = 16384
SEQS = 8


def block_scale(stream_key, extent, shards, least, largest):
    def one(axis_at, blocks):
        heights = jax.random.uniform(jax.random.fold_in(jax.random.fold_in(stream_key, 6), axis_at), (blocks,), jnp.float32, least / len(shards), largest / len(shards))
        return jnp.repeat(jnp.exp(heights), extent[axis_at] // blocks).reshape((-1,) + (1,) * (len(extent) - axis_at - 1))

    factor_of = one(*shards[0])
    for cut in shards[1:]:
        factor_of = factor_of * one(*cut)
    return factor_of


def scatter_about(stream_key, shape, spread, bound, split=(), kind=jnp.bfloat16):
    entries = jax.random.normal(stream_key, shape, jnp.float32) * spread
    if len(split) > 0:
        entries = block_scale(stream_key, shape, split, -0.22, 0.18) * entries
    return jnp.clip(entries, min=-bound, max=bound).astype(kind)


def setup_inputs(seed: int = 0) -> dict:
    arg_keys = jax.random.split(jax.random.key(seed), 9)
    u_pre = scatter_about(arg_keys[0], (SEQS, SEQLEN, SGU_W), 1.0, 6.0, ((0, 8), (1, 16)))
    v_pre = scatter_about(arg_keys[1], (SEQS, SEQLEN, SGU_W), 1.0, 6.0, ((0, 8), (1, 16)))
    d_out = scatter_about(arg_keys[2], (SEQS, SEQLEN, D), 1.0, 6.0, ((0, 8), (1, 16)))
    w_mix = scatter_about(arg_keys[3], (GROUPS, BLOCK, BLOCK), BLOCK ** -0.5, 0.5)
    mix_bias = jnp.clip(1.0 + 0.18 * jax.random.normal(arg_keys[4], (GROUPS, BLOCK), jnp.float32), 0.1, 1.9)
    norm_gain = jnp.clip(1.0 + 0.18 * jax.random.normal(arg_keys[5], (GROUPS, CHANS), jnp.float32), 0.1, 1.9)
    norm_shift = scatter_about(arg_keys[6], (GROUPS, CHANS), 0.5, 3.0, (), jnp.float32)
    w_out = scatter_about(arg_keys[7], (SGU_W, D), SGU_W ** -0.5, 0.125, ((0, 8),))
    return {"u_pre": u_pre, "v_pre": v_pre, "d_out": d_out, "w_mix": w_mix, "mix_bias": mix_bias, "norm_gain": norm_gain, "norm_shift": norm_shift, "w_out": w_out}


EPS = 1e-05

def mechanism(grad_s, u_pre, v_pre, w_mix, mix_bias, gain, shift):
    items, length, width = grad_s.shape
    groups, span = (w_mix.shape[0], w_mix.shape[1])
    chans = width // groups
    shape = (items, length // span, span, groups, chans)
    u_val = u_pre.astype(jnp.float32).reshape(shape)
    v_val = v_pre.astype(jnp.float32).reshape(shape)
    cotan = grad_s.astype(jnp.float32).reshape(shape)
    upper, u_back = jax.vjp(jax.nn.gelu, u_val)
    gated, v_back = jax.vjp(jax.nn.gelu, v_val)
    centre = gated - lax.optimization_barrier(jnp.mean(gated, axis=-1, keepdims=True))
    inverse = lax.rsqrt(lax.optimization_barrier(jnp.mean(centre * centre, axis=-1, keepdims=True)) + EPS)
    scaled = centre * inverse
    normed = (scaled * gain + shift).astype(jnp.bfloat16)
    lower = jnp.tril(jnp.ones((span, span), dtype=bool))
    w_low = jnp.where(lower[None], w_mix, jnp.zeros_like(w_mix))
    mixed = jnp.einsum('gts,insgc->intgc', w_low.astype(jnp.float32), normed.astype(jnp.float32))
    mixed = mixed + jnp.transpose(mix_bias)[:, :, None]
    gated_out = (upper * mixed).astype(jnp.bfloat16)
    d_mixed = cotan * upper
    d_mixed_b = d_mixed.astype(jnp.bfloat16)
    grad_u = u_back(cotan * mixed)[0].astype(jnp.bfloat16).reshape(items, length, width)
    grad_bias = jnp.transpose(lax.optimization_barrier(jnp.sum(d_mixed, axis=(0, 1, 4))))
    grad_w = jnp.einsum('intgc,insgc->gts', d_mixed_b.astype(jnp.float32), normed.astype(jnp.float32))
    grad_w = jnp.where(lower[None], grad_w, jnp.zeros_like(grad_w))
    d_normed = jnp.einsum('gts,intgc->insgc', w_low.astype(jnp.float32), d_mixed_b.astype(jnp.float32))
    grad_gain = lax.optimization_barrier(jnp.sum(d_normed * scaled, axis=(0, 1, 2)))
    grad_shift = lax.optimization_barrier(jnp.sum(d_normed, axis=(0, 1, 2)))
    d_scaled = d_normed * gain
    d_gated = inverse * (d_scaled - lax.optimization_barrier(jnp.mean(d_scaled, axis=-1, keepdims=True)) - scaled * lax.optimization_barrier(jnp.mean(d_scaled * scaled, axis=-1, keepdims=True)))
    grad_v = v_back(d_gated)[0].astype(jnp.bfloat16).reshape(items, length, width)
    return (grad_u, grad_v, gated_out.reshape(items, length, width), grad_w, grad_bias, grad_gain, grad_shift)

def reference(u_pre, v_pre, d_out, w_mix, mix_bias, norm_gain, norm_shift, w_out):
    flat_d = d_out.reshape(-1, D)
    grad_s = jnp.dot(flat_d, jnp.transpose(w_out), preferred_element_type=jnp.float32)
    grad_s = grad_s.astype(jnp.bfloat16).reshape(SEQS, SEQLEN, SGU_W)

    def one_sequence(packed):
        cot, upre, vpre = packed
        return mechanism(cot[None], upre[None], vpre[None], w_mix, mix_bias, norm_gain, norm_shift)
    grad_u, grad_v, gated_out, grad_w, grad_bias, grad_gain, grad_shift = lax.map(one_sequence, (grad_s, u_pre, v_pre))
    grad_u = grad_u.reshape(SEQS, SEQLEN, SGU_W)
    grad_v = grad_v.reshape(SEQS, SEQLEN, SGU_W)
    flat_s = gated_out.reshape(-1, SGU_W)
    grad_w_out = jnp.dot(jnp.transpose(flat_s), flat_d, preferred_element_type=jnp.float32)
    return (grad_u, grad_v, grad_w_out, lax.optimization_barrier(jnp.sum(grad_w, axis=0)), lax.optimization_barrier(jnp.sum(grad_bias, axis=0)), lax.optimization_barrier(jnp.sum(grad_gain, axis=0)), lax.optimization_barrier(jnp.sum(grad_shift, axis=0)))
```

```python
import functools

import jax
import jax.numpy as jnp
from jax import lax
from jax.experimental import pallas as pl
from jax.experimental.pallas import tpu as pltpu
from jax.sharding import PartitionSpec as P

EPS = 1e-05
C0 = 0.7978845608028654
C1 = 0.044715
F32 = jnp.float32
BF = jnp.bfloat16
MESH = pl.DeviceIdType.MESH
WID = 2048
EXT = WID + 128


def rdma(src, dst, ssem, rsem, dev):
    return pltpu.make_async_remote_copy(
        src_ref=src, dst_ref=dst, send_sem=ssem, recv_sem=rsem, device_id=dev, device_id_type=MESH
    )


def al(v, m):
    return pl.multiple_of(v, m)


def gelu_pair(a):
    a2 = a * a
    th = jnp.tanh(a * (C0 + (C0 * C1) * a2))
    s = 0.5 + 0.5 * th
    g = a * s
    slope = s + g * (1.0 - s) * (2.0 * C0 + (6.0 * C0 * C1) * a2)
    return g, slope


def lane_mean(a):
    return jnp.sum(a, axis=-1, keepdims=True) * (1.0 / 128.0)


def dot_nn(a, b):
    return lax.dot_general(a, b, (((1,), (0,)), ((), ())), preferred_element_type=F32)


def dot_nt(a, b):
    return lax.dot_general(a, b, (((1,), (1,)), ((), ())), preferred_element_type=F32)


def kernel(
    u_hbm, v_hbm, d_hbm, wm_ref, bias_ref, gain_ref, shift_ref, w_hbm,
    gu_hbm, gv_hbm, gw_hbm, gm_hbm, gb_ref, gg_ref, gsh_ref,
    d_v, wbuf, ub, vb, gub, gvb, gs, gt, pb, pr, tb, r1, q, r2, vx, rx, ob, of,
    cb, rc1, qc, rc2, qd, rc3, cg, cp, gm,
    st, st2, rs0, rs1, wl, wlt, bb, gwacc, bacc, gacc, sacc,
    ld_s, uv_s, out_s, wsend, wrecv, wrel_s, wrel_r,
    ps_s, ps_r, s1_s, s1_r, s2_s, s2_r, x_s, x_r, g1_s, g1_r, g2_s, g2_r,
    c_s, c_r, t_s, t_r, fin_s,
):
    sp = lax.axis_index("sp")
    dp = lax.axis_index("dp")
    z, y = sp // 4, sp % 4
    x, c = dp // 2, dp % 2
    o = 1 - c

    def dev(x_, y_, z_, c_):
        return (z_ * 4 + y_, x_ * 2 + c_)

    def px(d):
        return dev((x + d) % 4, y, z, c)

    def py(d):
        return dev(x, (y + d) % 4, z, c)

    def pz(d):
        return dev(x, y, (z + d) % 4, c)

    mate = dev(x, y, z, o)
    first = (py, pz)
    second = (pz, py)
    i1 = (y, z)
    i2 = (z, y)

    own = [
        pltpu.make_async_copy(w_hbm.at[pl.ds(g * 128, 128)], wbuf.at[g, c], ld_s.at[g]) for g in range(2)
    ]
    dcp = [
        pltpu.make_async_copy(
            d_hbm.at[0, pl.ds(i * 256, 256)], d_v.at[pl.ds(i * 256, 256)], ld_s.at[2 + i]
        )
        for i in range(4)
    ]
    for cpy in own:
        cpy.start()
    for cpy in dcp:
        cpy.start()

    def unit(u):
        par = u % 2
        quad = u // 2
        base = jnp.where(quad == 1, 3, jnp.where(quad == 2, 1, jnp.where(quad == 3, 2, 0)))
        xu = (x + base + par * quad * (3 - quad)) % 4
        return xu, par, quad

    def cols(u, cls):
        xu, par, _ = unit(u)
        return pl.ds(al((4 * xu + 2 * cls + par) * 128, 128), 128)

    def uv_copies(u):
        slot = u % 2
        res = []
        for k, (hbm, buf) in enumerate(((u_hbm, ub), (v_hbm, vb))):
            for cls in range(2):
                res.append(
                    pltpu.make_async_copy(
                        hbm.at[0, :, cols(u, cls)],
                        buf.at[slot, :, pl.ds(cls * 128, 128)],
                        uv_s.at[slot, k, cls],
                    )
                )
        return res

    def out_copies(u):
        slot = u % 2
        res = []
        for k, (hbm, buf) in enumerate(((gu_hbm, gub), (gv_hbm, gvb))):
            for cls in range(2):
                res.append(
                    pltpu.make_async_copy(
                        buf.at[slot, :, pl.ds(cls * 128, 128)],
                        hbm.at[0, :, cols(u, cls)],
                        out_s.at[slot, k, cls],
                    )
                )
        return res

    for cpy in uv_copies(0):
        cpy.start()

    barrier = pltpu.get_barrier_semaphore()
    for peer in [mate] + [f(d) for f in (px, py, pz) for d in (1, 2, 3)]:
        pl.semaphore_signal(barrier, inc=1, device_id=peer, device_id_type=MESH)
    pl.semaphore_wait(barrier, 10)

    def wx(k):
        src, dst, d = ((0, 2, 1), (1, 3, 3), (1, 5, 1), (0, 4, 3), (2, 6, 1), (3, 7, 3))[k]
        return rdma(wbuf.at[src, c], wbuf.at[dst, c], wsend.at[k], wrecv.at[k], px(d))

    arrival = {2: 0, 3: 1, 5: 2, 4: 3, 6: 4, 7: 5}

    def relay(s, k):
        return rdma(wbuf.at[s, k], wbuf.at[s, k], wrel_s.at[s], wrel_r.at[s], mate)

    for cpy in own:
        cpy.wait()
    relay(0, c).start()
    relay(1, c).start()
    for k in range(4):
        wx(k).start()

    tri = lax.broadcasted_iota(jnp.int32, (128, 128), 0) >= lax.broadcasted_iota(jnp.int32, (128, 128), 1)

    def prep(g, _):
        w = jnp.where(tri, wm_ref[g].astype(F32), 0.0)
        wl[g] = w.astype(BF)
        wlt[g] = w.T.astype(BF)
        row = bias_ref[pl.ds(g, 1), :]
        bb[g] = jnp.broadcast_to(row, (128, 128)).T
        return 0

    lax.fori_loop(0, 16, prep, 0)
    for cpy in dcp:
        cpy.wait()

    def ps(u):
        return rdma(pb.at[u % 2, o], pr.at[u], ps_s.at[u % 2], ps_r.at[u], mate)

    def s1(u, ab, d, j):
        return rdma(
            tb.at[u % 2, pl.ds(al(32 * j, 32), 32), pl.ds(1024 * ab, 1024)],
            r1.at[u, ab, d - 1],
            s1_s.at[u % 2, ab, d - 1],
            s1_r.at[u, ab, d - 1],
            first[ab](d),
        )

    def s2(u, ab, d, j):
        return rdma(
            q.at[u % 2, ab, :, pl.ds(al(256 * j, 256), 256)],
            r2.at[u, ab, d - 1],
            s2_s.at[u % 2, ab, d - 1],
            s2_r.at[u, ab, d - 1],
            second[ab](d),
        )

    def xs(u):
        xu, par, quad = unit(u)
        return rdma(vx.at[u], rx.at[par, quad], x_s.at[u], x_r.at[par, quad], dev(xu, y, z, c))

    PAIRS = [(ab, d) for ab in range(2) for d in (1, 2, 3)]

    def do_ts(u):
        ps(u).wait()
        slot = u % 2
        xu, par, _ = unit(u)

        def body(i, _):
            r = pl.ds(al(i * 16, 16), 16)
            tb[slot, r, :] = (
                pb[slot, c, r, pl.ds(0, WID)].astype(F32) + pr[u, r, pl.ds(0, WID)].astype(F32)
            ).astype(BF)
            return 0

        lax.fori_loop(0, 8, body, 0)
        cb[xu * 2 + par] = (
            pb[slot, c, :, pl.ds(WID, 128)].astype(F32) + pr[u, :, pl.ds(WID, 128)].astype(F32)
        ).astype(BF)
        for ab, d in PAIRS:
            s1(u, ab, d, (i1[ab] + d) % 4).start()

    def do_s2(u):
        slot = u % 2
        for ab, d in PAIRS:
            s1(u, ab, d, (i1[ab] + d) % 4).wait()
        for ab in range(2):
            for h in range(2):
                r = pl.ds(16 * h, 16)
                acc = tb[slot, pl.ds(al(32 * i1[ab] + 16 * h, 16), 16), pl.ds(1024 * ab, 1024)].astype(F32)
                for k in range(3):
                    acc = acc + r1[u, ab, k, r, :].astype(F32)
                q[slot, ab, r, :] = acc.astype(BF)
        for ab, d in PAIRS:
            s2(u, ab, d, (i2[ab] + d) % 4).start()

    def do_x(u):
        slot = u % 2
        _, par, _ = unit(u)
        for ab, d in PAIRS:
            s2(u, ab, d, (i2[ab] + d) % 4).wait()
        for ab in range(2):
            acc = q[slot, ab, :, pl.ds(al(256 * i2[ab], 256), 256)].astype(F32)
            for k in range(3):
                acc = acc + r2[u, ab, k].astype(F32)
            vx[u, ab] = acc.astype(BF)

        @pl.when(u >= 2)
        def _():
            xs(u).start()

    def ob_small(g, ab, j):
        return ob.at[
            pl.ds(al(g * 128 + 32 * i1[ab], 32), 32), pl.ds(al(1024 * ab + 256 * j, 256), 256)
        ]

    def ob_big(g, ab, j):
        return ob.at[pl.ds(al(g * 128 + 32 * j, 32), 32), pl.ds(1024 * ab, 1024)]

    def g1(g, ab, d, j):
        return rdma(
            ob_small(g, ab, j), ob_small(g, ab, j), g1_s.at[g, ab, d - 1], g1_r.at[g, ab, d - 1], second[ab](d)
        )

    def g2(g, ab, d, j):
        return rdma(
            ob_big(g, ab, j), ob_big(g, ab, j), g2_s.at[g, ab, d - 1], g2_r.at[g, ab, d - 1], first[ab](d)
        )

    def do_f(g):
        for k in (1, 2, 3):
            rdma(vx.at[g], rx.at[g, k], x_s.at[g], x_r.at[g, k], mate).wait_recv()
        for ab in range(2):
            acc = vx[g, ab].astype(F32)
            for k in (1, 2, 3):
                acc = acc + rx[g, k, ab].astype(F32)
            ob_small(g, ab, i2[ab])[...] = acc.astype(BF)
        for ab, d in PAIRS:
            g1(g, ab, d, i2[ab]).start()

    def do_g2(g):
        for ab, d in PAIRS:
            g1(g, ab, d, (i2[ab] + 4 - d) % 4).wait_recv()
        for ab, d in PAIRS:
            g2(g, ab, d, i1[ab]).start()

    def out_w(g):
        return pltpu.make_async_copy(
            of.at[pl.ds(g * 128, 128)], gw_hbm.at[pl.ds(g * 128, 128)], fin_s.at[g]
        )

    def do_out(g):
        for ab, d in PAIRS:
            g2(g, ab, d, (i1[ab] + 4 - d) % 4).wait_recv()

        def body(i, _):
            r = pl.ds(al(g * 128 + i * 16, 16), 16)
            of[r, :] = ob[r, :].astype(F32)
            return 0

        lax.fori_loop(0, 8, body, 0)
        out_w(g).start()

    def arrive(s):
        wx(arrival[s]).wait_recv()
        relay(s, c).start()

    def unit_body(u, _):
        slot = u % 2
        xu, par, _q = unit(u)
        relay(u, o).wait_recv()

        @pl.when(u < 7)
        def _():
            for cpy in uv_copies(u + 1):
                cpy.start()

        def gs_body(i, _):
            r = pl.ds(al(i * 512, 512), 512)
            gs[r, :] = dot_nt(d_v[r, :], wbuf[u].reshape(256, WID)).astype(BF)
            return 0

        lax.fori_loop(0, 2, gs_body, 0)

        @pl.when(u >= 2)
        def _():
            do_x(u - 2)

        @pl.when(u >= 1)
        def _():
            do_ts(u - 1)

        for cpy in uv_copies(u):
            cpy.wait()

        @pl.when(u >= 2)
        def _():
            for cpy in out_copies(u - 2):
                cpy.wait()

        gwacc[...] = jnp.zeros_like(gwacc)
        bacc[...] = jnp.zeros_like(bacc)
        gacc[...] = jnp.zeros_like(gacc)
        sacc[...] = jnp.zeros_like(sacc)

        def block(n, _):
            r = pl.ds(al(n * 128, 128), 128)
            for cls in range(2):
                grp = 4 * xu + 2 * cls + par
                ln = pl.ds(cls * 128, 128)
                gain = gain_ref[pl.ds(grp, 1), :]
                shift = shift_ref[pl.ds(grp, 1), :]
                gated, v_slope = gelu_pair(vb[slot, r, ln].astype(F32))
                cen = gated - lane_mean(gated)
                inv = lax.rsqrt(lane_mean(cen * cen) + EPS)
                scaled = cen * inv
                nb = (scaled * gain + shift).astype(BF)
                upper, u_slope = gelu_pair(ub[slot, r, ln].astype(F32))
                cot = gs[r, ln].astype(F32)
                dm = cot * upper
                dmb = dm.astype(BF)
                bacc[cls] += dm
                mixed = dot_nn(wl[grp], nb) + bb[grp]
                dn = dot_nn(wlt[grp], dmb)
                gwacc[cls] += dot_nt(dmb, nb)
                gt[pl.ds(cls * 128, 128), r] = (upper * mixed).T.astype(BF)
                gub[slot, r, ln] = (cot * mixed * u_slope).astype(BF)
                prod = dn * scaled
                gacc[cls] += jnp.sum(prod.reshape(16, 8, 128), axis=0)
                sacc[cls] += jnp.sum(dn.reshape(16, 8, 128), axis=0)
                e = dn * gain
                m1 = lane_mean(e)
                m2 = lane_mean(prod * gain)
                gvb[slot, r, ln] = ((e - m1 - scaled * m2) * (v_slope * inv)).astype(BF)
            return 0

        lax.fori_loop(0, 8, block, 0)
        for cpy in out_copies(u):
            cpy.start()

        @pl.when(u >= 1)
        def _():
            do_s2(u - 1)

        def p_body(j, _):
            cl = pl.ds(al(j * 256, 256), 256)
            pb[slot, :, :, cl] = dot_nn(gt[...], d_v[:, cl]).astype(BF).reshape(2, 128, 256)
            return 0

        lax.fori_loop(0, 8, p_body, 0)
        for cls in range(2):
            grp = 4 * xu + 2 * cls + par
            pb[slot, cls, :, pl.ds(WID, 128)] = jnp.where(tri, gwacc[cls], 0.0).astype(BF)
            st[0, pl.ds(grp, 1), :] = jnp.sum(bacc[cls].T, axis=0, keepdims=True)
            st[1, pl.ds(grp, 1), :] = jnp.sum(gacc[cls], axis=0, keepdims=True)
            st[2, pl.ds(grp, 1), :] = jnp.sum(sacc[cls], axis=0, keepdims=True)
        ps(u).start()

        @pl.when(u == 1)
        def _():
            arrive(2)
            wx(4).start()
            arrive(3)
            wx(5).start()

        @pl.when(u == 3)
        def _():
            arrive(4)
            arrive(5)

        @pl.when(u == 5)
        def _():
            arrive(6)
            arrive(7)

        return 0

    lax.fori_loop(0, 8, unit_body, 0)

    def stat_sum(src, parts, dst):
        acc = src[...]
        for part in parts:
            acc = acc + part[...]
        dst[...] = acc

    t0 = rdma(st, rs0, t_s.at[0, 0], t_r.at[0, 0], mate)
    t0.start()

    def tstage(k, d, src, f):
        return rdma(src, rs1.at[k, d - 1], t_s.at[k + 1, d - 1], t_r.at[k + 1, d - 1], f(d))

    def cy(d, j):
        return rdma(
            cb.at[:, pl.ds(al(32 * j, 32), 32)], rc1.at[d - 1], c_s.at[0, d - 1], c_r.at[0, d - 1], py(d)
        )

    def cz(d, j):
        return rdma(qc.at[pl.ds(2 * j, 2)], rc2.at[d - 1], c_s.at[1, d - 1], c_r.at[1, d - 1], pz(d))

    def cx(d):
        return rdma(qd, rc3.at[d - 1], c_s.at[2, d - 1], c_r.at[2, d - 1], px(d))

    def cgz(d, j):
        ref = cg.at[pl.ds(2 * j, 2), pl.ds(al(32 * y, 32), 32)]
        return rdma(ref, ref, c_s.at[3, d - 1], c_r.at[3, d - 1], pz(d))

    def cgy(d, j):
        ref = cg.at[:, pl.ds(al(32 * j, 32), 32)]
        return rdma(ref, ref, c_s.at[4, d - 1], c_r.at[4, d - 1], py(d))

    DS = (1, 2, 3)
    do_x(6)
    do_ts(7)
    for d in DS:
        cy(d, (y + d) % 4).start()
    t0.wait()
    stat_sum(st, [rs0], st2.at[0])
    for d in DS:
        tstage(0, d, st2.at[0], py).start()
    do_f(0)
    do_s2(7)
    for d in DS:
        cy(d, (y + d) % 4).wait()
    acc = cb[:, pl.ds(al(32 * y, 32), 32), :].astype(F32)
    for k in range(3):
        acc = acc + rc1[k].astype(F32)
    qc[...] = acc.astype(BF)
    for d in DS:
        cz(d, (z + d) % 4).start()
    for d in DS:
        tstage(0, d, st2.at[0], py).wait()
    stat_sum(st2.at[0], [rs1.at[0, k] for k in range(3)], st2.at[1])
    for d in DS:
        tstage(1, d, st2.at[1], pz).start()
    do_g2(0)
    do_x(7)
    for d in DS:
        cz(d, (z + d) % 4).wait()
    acc = qc[pl.ds(2 * z, 2)].astype(F32)
    for k in range(3):
        acc = acc + rc2[k].astype(F32)
    qd[...] = acc.astype(BF)
    for d in DS:
        cx(d).start()
    for d in DS:
        tstage(1, d, st2.at[1], pz).wait()
    stat_sum(st2.at[1], [rs1.at[1, k] for k in range(3)], st2.at[2])
    for d in DS:
        tstage(2, d, st2.at[2], px).start()
    do_f(1)
    for d in DS:
        cx(d).wait()
    acc = qd[...].astype(F32)
    for k in range(3):
        acc = acc + rc3[k].astype(F32)
    cg[pl.ds(2 * z, 2), pl.ds(al(32 * y, 32), 32), :] = acc.astype(BF)
    for d in DS:
        cgz(d, z).start()
    do_out(0)
    for d in DS:
        tstage(2, d, st2.at[2], px).wait()
    tot = st2[2]
    for k in range(3):
        tot = tot + rs1[2, k]
    gb_ref[...] = tot[0]
    gg_ref[...] = tot[1]
    gsh_ref[...] = tot[2]
    do_g2(1)
    for d in DS:
        cgz(d, (z + 4 - d) % 4).wait_recv()
    for d in DS:
        cgy(d, y).start()
    for d in DS:
        cgy(d, (y + 4 - d) % 4).wait_recv()
    swap = rdma(cg, cp, c_s.at[5, 0], c_r.at[5, 0], mate)
    swap.start()

    def gm_body(src, cls):
        def body(i, _):
            gm[(i // 2) * 4 + 2 * cls + i % 2] = src[i].astype(F32)
            return 0

        lax.fori_loop(0, 8, body, 0)

    gm_body(cg, c)
    do_out(1)
    swap.wait()
    gm_body(cp, o)
    gmc = pltpu.make_async_copy(gm, gm_hbm, fin_s.at[2])
    gmc.start()

    for k in range(6):
        wx(k).wait_send()
    for s in range(8):
        relay(s, c).wait_send()
    for u in range(2, 8):
        xs(u).wait_send()
    for g in range(2):
        for ab, d in PAIRS:
            g1(g, ab, d, i2[ab]).wait_send()
            g2(g, ab, d, i1[ab]).wait_send()
    for d in DS:
        cgz(d, z).wait_send()
        cgy(d, y).wait_send()
    for u in (6, 7):
        for cpy in out_copies(u):
            cpy.wait()
    out_w(0).wait()
    out_w(1).wait()
    gmc.wait()


def on_device(u_pre, v_pre, d_out, w_mix, mix_bias, norm_gain, norm_shift, w_out):
    hbm = pl.BlockSpec(memory_space=pl.ANY)
    vm = pl.BlockSpec(memory_space=pltpu.VMEM)
    V = pltpu.VMEM
    DMA = pltpu.SemaphoreType.DMA
    scratch = [
        V((1024, WID), BF), V((8, 2, 128, WID), BF),
        V((2, 1024, 256), BF), V((2, 1024, 256), BF), V((2, 1024, 256), BF), V((2, 1024, 256), BF),
        V((1024, 256), BF), V((256, 1024), BF),
        V((2, 2, 128, EXT), BF), V((8, 128, EXT), BF), V((2, 128, WID), BF),
        V((8, 2, 3, 32, 1024), BF), V((2, 2, 32, 1024), BF), V((8, 2, 3, 32, 256), BF),
        V((8, 2, 32, 256), BF), V((2, 4, 2, 32, 256), BF), V((256, WID), BF), V((256, WID), F32),
        V((8, 128, 128), BF), V((3, 8, 32, 128), BF), V((8, 32, 128), BF), V((3, 2, 32, 128), BF),
        V((2, 32, 128), BF), V((3, 2, 32, 128), BF), V((8, 128, 128), BF), V((8, 128, 128), BF),
        V((16, 128, 128), F32),
        V((3, 16, 128), F32), V((3, 3, 16, 128), F32), V((3, 16, 128), F32), V((3, 3, 3, 16, 128), F32),
        V((16, 128, 128), BF), V((16, 128, 128), BF), V((16, 128, 128), F32),
        V((2, 128, 128), F32), V((2, 128, 128), F32), V((2, 8, 128), F32), V((2, 8, 128), F32),
        DMA((6,)), DMA((2, 2, 2)), DMA((2, 2, 2)), DMA((6,)), DMA((6,)), DMA((8,)), DMA((8,)),
        DMA((2,)), DMA((8,)), DMA((2, 2, 3)), DMA((8, 2, 3)), DMA((2, 2, 3)), DMA((8, 2, 3)),
        DMA((8,)), DMA((2, 4)), DMA((2, 2, 3)), DMA((2, 2, 3)), DMA((2, 2, 3)), DMA((2, 2, 3)),
        DMA((6, 3)), DMA((6, 3)), DMA((4, 3)), DMA((4, 3)), DMA((3,)),
    ]
    outs = pl.pallas_call(
        kernel,
        out_shape=(
            jax.ShapeDtypeStruct(u_pre.shape, BF),
            jax.ShapeDtypeStruct(v_pre.shape, BF),
            jax.ShapeDtypeStruct((256, WID), F32),
            jax.ShapeDtypeStruct((16, 128, 128), F32),
            jax.ShapeDtypeStruct((16, 128), F32),
            jax.ShapeDtypeStruct((16, 128), F32),
            jax.ShapeDtypeStruct((16, 128), F32),
        ),
        in_specs=[hbm, hbm, hbm, vm, vm, vm, vm, hbm],
        out_specs=(hbm, hbm, hbm, hbm, vm, vm, vm),
        scratch_shapes=scratch,
        compiler_params=pltpu.CompilerParams(
            collective_id=0, has_side_effects=True, vmem_limit_bytes=60 * 1024 * 1024
        ),
    )(u_pre, v_pre, d_out, w_mix, mix_bias, norm_gain, norm_shift, w_out)
    return outs


def solution(mesh):
    return jax.shard_map(
        on_device,
        mesh=mesh,
        in_specs=(
            P("dp", "sp", None), P("dp", "sp", None), P("dp", "sp", None),
            P(), P(), P(), P(), P("dp", None),
        ),
        out_specs=(P("dp", "sp", None), P("dp", "sp", None), P("dp", None), P(), P(), P(), P()),
        check_vma=False,
    )
```

```python
import functools

import jax
import jax.numpy as jnp
from jax import lax
from jax.experimental import pallas as pl
from jax.experimental.pallas import tpu as pltpu
from jax.sharding import PartitionSpec as P

EPS = 1e-05
C0 = 0.7978845608028654
C1 = 0.044715
F32 = jnp.float32
BF = jnp.bfloat16
MESH = pl.DeviceIdType.MESH
WID = 2048
EXT = WID + 128


def rdma(src, dst, ssem, rsem, dev):
    return pltpu.make_async_remote_copy(
        src_ref=src, dst_ref=dst, send_sem=ssem, recv_sem=rsem, device_id=dev, device_id_type=MESH
    )


def al(v, m):
    return pl.multiple_of(v, m)


def gelu_pair(a):
    a2 = a * a
    th = jnp.tanh(a * (C0 + (C0 * C1) * a2))
    s = 0.5 + 0.5 * th
    g = a * s
    slope = s + g * (1.0 - s) * (2.0 * C0 + (6.0 * C0 * C1) * a2)
    return g, slope


def gelu_value(a):
    return a * (0.5 + 0.5 * jnp.tanh(a * (C0 + (C0 * C1) * (a * a))))


def gelu_slope(a):
    return gelu_pair(a)[1]


def lane_mean(a):
    return jnp.sum(a, axis=-1, keepdims=True) * (1.0 / 128.0)


def dot_nn(a, b):
    return lax.dot_general(a, b, (((1,), (0,)), ((), ())), preferred_element_type=F32)


def dot_nt(a, b):
    return lax.dot_general(a, b, (((1,), (1,)), ((), ())), preferred_element_type=F32)


def kernel(
    u_hbm, v_hbm, d_hbm, wm_hbm, bias_hbm, gain_hbm, shift_hbm, w_hbm,
    gu_ref, gv_ref, gw_ref, gm_ref, stat_ref,
    d_v, wbuf, ub, vb, gs, gt, pb, pr, tb, ra, rb, q, rc, rd, vx, rx, ob,
    qc, rc2, qd, rc3, cg, cp,
    st, st2, rs0, rs1, bias_ref, gain_ref, shift_ref, wl, wlt, bb, gwacc, bacc, gacc, sacc,
    sinv, sdn,
    ld_s, uv_s, wsend, wrecv, wrel_s, wrel_r,
    ps_s, ps_r, s1_s, s1_r, s2_s, s2_r, x_s, x_r, g1_s, g1_r, g2_s, g2_r,
    c_s, c_r, t_s, t_r,
):
    sp = lax.axis_index("sp")
    dp = lax.axis_index("dp")
    z, y = sp // 4, sp % 4
    x, c = dp // 2, dp % 2
    o = 1 - c

    def dev(x_, y_, z_, c_):
        return (z_ * 4 + y_, x_ * 2 + c_)

    def px(d):
        return dev((x + d) % 4, y, z, c)

    def py(d):
        return dev(x, (y + d) % 4, z, c)

    def pz(d):
        return dev(x, y, (z + d) % 4, c)

    mate = dev(x, y, z, o)
    first = (py, pz)
    second = (pz, py)
    i1 = (y, z)
    i2 = (z, y)

    own = [
        pltpu.make_async_copy(w_hbm.at[pl.ds(g * 128, 128)], wbuf.at[g, c], ld_s.at[g]) for g in range(2)
    ]
    dcp = [
        pltpu.make_async_copy(
            d_hbm.at[0, pl.ds(i * 256, 256)], d_v.at[pl.ds(i * 256, 256)], ld_s.at[2 + i]
        )
        for i in range(4)
    ]
    for cpy in own:
        cpy.start()
    params = [
        pltpu.make_async_copy(a, b, ld_s.at[6 + i])
        for i, (a, b) in enumerate(
            ((wm_hbm, wl), (bias_hbm, bias_ref), (gain_hbm, gain_ref), (shift_hbm, shift_ref))
        )
    ]
    for cpy in params:
        cpy.start()
    for cpy in dcp:
        cpy.start()

    def unit(u):
        par = u % 2
        quad = u // 2
        base = jnp.where(quad == 1, 3, jnp.where(quad == 2, 1, jnp.where(quad == 3, 2, 0)))
        xu = (x + base + par * quad * (3 - quad)) % 4
        return xu, par, quad

    def cols(u, cls):
        xu, par, _ = unit(u)
        return pl.ds(al((4 * xu + 2 * cls + par) * 128, 128), 128)

    def uv_copies(u):
        slot = u % 2
        res = []
        for k, (hbm, buf) in enumerate(((u_hbm, ub), (v_hbm, vb))):
            for cls in range(2):
                res.append(
                    pltpu.make_async_copy(
                        hbm.at[0, :, cols(u, cls)],
                        buf.at[slot, :, pl.ds(cls * 128, 128)],
                        uv_s.at[slot, k, cls],
                    )
                )
        return res

    for cpy in uv_copies(0):
        cpy.start()

    barrier = pltpu.get_barrier_semaphore()
    for peer in [mate] + [f(d) for f in (px, py, pz) for d in (1, 2, 3)]:
        pl.semaphore_signal(barrier, inc=1, device_id=peer, device_id_type=MESH)
    pl.semaphore_wait(barrier, 10)

    def wx(k):
        src, dst, d = ((0, 2, 1), (1, 3, 3), (1, 5, 1), (0, 4, 3), (2, 6, 1), (3, 7, 3))[k]
        return rdma(wbuf.at[src, c], wbuf.at[dst, c], wsend.at[k], wrecv.at[k], px(d))

    arrival = {2: 0, 3: 1, 5: 2, 4: 3, 6: 4, 7: 5}

    def relay(s, k):
        return rdma(wbuf.at[s, k], wbuf.at[s, k], wrel_s.at[s], wrel_r.at[s], mate)

    for cpy in own:
        cpy.wait()
    relay(0, c).start()
    relay(1, c).start()
    for k in range(4):
        wx(k).start()

    tri = lax.broadcasted_iota(jnp.int32, (128, 128), 0) >= lax.broadcasted_iota(jnp.int32, (128, 128), 1)

    def prep(g, _):
        w = jnp.where(tri, wl[g].astype(F32), 0.0)
        wl[g] = w.astype(BF)
        wlt[g] = w.T.astype(BF)
        return 0

    for cpy in params:
        cpy.wait()
    lax.fori_loop(0, 16, prep, 0)
    for cpy in dcp:
        cpy.wait()

    def ps(u):
        return rdma(pb.at[u % 2, o], pr.at[u % 2], ps_s.at[u % 2], ps_r.at[u], mate)

    WAB = (1152, 1024)
    OFF = (0, 1152)

    def rows(j, half=None):
        if half is None:
            return pl.ds(al(32 * j, 32), 32)
        return pl.ds(al(32 * j + 16 * half, 16), 16)

    def lanes(j):
        return pl.ds(al(256 * j, 256), 256)

    HOP = (1, 3)

    def s1a(u, ab, k):
        w = WAB[ab]
        return rdma(
            tb.at[u % 4, rows((i1[ab] + 2) % 4, k), pl.ds(OFF[ab], w)],
            ra.at[u, ab, k, :, pl.ds(0, w)],
            s1_s.at[u % 4, 0, ab, k], s1_r.at[u, 0, ab, k], first[ab](HOP[k]),
        )

    def s1b(u, ab, k):
        w = WAB[ab]
        return rdma(
            tb.at[u % 4, rows((i1[ab] + HOP[k]) % 4), pl.ds(OFF[ab], w)],
            rb.at[u, ab, k, :, pl.ds(0, w)],
            s1_s.at[u % 4, 1, ab, k], s1_r.at[u, 1, ab, k], first[ab](HOP[k]),
        )

    def s2a(u, ab, k):
        return rdma(
            q.at[u % 4, ab, pl.ds(16 * k, 16), lanes((i2[ab] + 2) % 4)],
            rc.at[u, ab, k],
            s2_s.at[u % 4, 0, ab, k], s2_r.at[u, 0, ab, k], second[ab](HOP[k]),
        )

    def s2b(u, ab, k):
        return rdma(
            q.at[u % 4, ab, :, lanes((i2[ab] + HOP[k]) % 4)],
            rd.at[u, ab, k],
            s2_s.at[u % 4, 1, ab, k], s2_r.at[u, 1, ab, k], second[ab](HOP[k]),
        )

    def xs(u):
        xu, par, quad = unit(u)
        return rdma(vx.at[u], rx.at[par, quad], x_s.at[u], x_r.at[par, quad], dev(xu, y, z, c))

    PAIRS = [(ab, d) for ab in range(2) for d in (1, 2, 3)]
    BOTH = [(ab, k) for ab in range(2) for k in range(2)]

    def do_ts(u):
        ps(u).wait()
        slot = u % 4

        def body(i, _):
            r = pl.ds(al(i * 16, 16), 16)
            for src, dst, w in ((0, 0, 1024), (WID, 1024, 128), (1024, 1152, 1024)):
                tb[slot, r, pl.ds(dst, w)] = (
                    pb[u % 2, c, r, pl.ds(src, w)].astype(F32) + pr[u % 2, r, pl.ds(src, w)].astype(F32)
                ).astype(BF)
            return 0

        lax.fori_loop(0, 8, body, 0)
        for ab, k in BOTH:
            s1a(u, ab, k).start()

    def do_s1b(u):
        slot = u % 4
        for ab, k in BOTH:
            s1a(u, ab, k).wait_recv()
        for ab, k in BOTH:
            r, ln = rows((i1[ab] + HOP[k]) % 4, k), pl.ds(OFF[ab], WAB[ab])
            tb[slot, r, ln] = (
                tb[slot, r, ln].astype(F32) + ra[u, ab, k, :, pl.ds(0, WAB[ab])].astype(F32)
            ).astype(BF)
        for ab, k in BOTH:
            s1b(u, ab, k).start()

    def do_s2a(u):
        slot = u % 4
        xu, par, _ = unit(u)
        for ab, k in BOTH:
            s1a(u, ab, k).wait_send()
            s1b(u, ab, k).wait()
        for ab in range(2):
            for h in range(2):
                hs = pl.ds(16 * h, 16)

                def total(a, w):
                    acc = tb[slot, rows(i1[ab], h), pl.ds(OFF[ab] + a, w)].astype(F32)
                    for k in range(2):
                        acc = acc + rb[u, ab, k, hs, pl.ds(a, w)].astype(F32)
                    return acc.astype(BF)

                q[slot, ab, hs, :] = total(0, 1024)
                if ab == 0:
                    qc[xu * 2 + par, hs, :] = total(1024, 128)
        for ab, k in BOTH:
            s2a(u, ab, k).start()

    def do_s2b(u):
        slot = u % 4
        for ab, k in BOTH:
            s2a(u, ab, k).wait_recv()
        for ab, k in BOTH:
            hs, ln = pl.ds(16 * k, 16), lanes((i2[ab] + HOP[k]) % 4)
            q[slot, ab, hs, ln] = (q[slot, ab, hs, ln].astype(F32) + rc[u, ab, k].astype(F32)).astype(BF)
        for ab, k in BOTH:
            s2b(u, ab, k).start()

    def do_x(u):
        slot = u % 4
        for ab, k in BOTH:
            s2a(u, ab, k).wait_send()
            s2b(u, ab, k).wait()
        for ab in range(2):
            acc = q[slot, ab, :, lanes(i2[ab])].astype(F32)
            for k in range(2):
                acc = acc + rd[u, ab, k].astype(F32)
            vx[u, ab] = acc.astype(BF)

        @pl.when(u >= 2)
        def _():
            xs(u).start()

    def ob_small(g, ab, j):
        return ob.at[
            pl.ds(al(g * 128 + 32 * i1[ab], 32), 32), pl.ds(al(1024 * ab + 256 * j, 256), 256)
        ]

    def ob_big(g, ab, j, half=None):
        r = pl.ds(al(g * 128 + 32 * j, 32), 32)
        if half is not None:
            r = pl.ds(al(g * 128 + 32 * j + 16 * half, 16), 16)
        return ob.at[r, pl.ds(1024 * ab, 1024)]

    def g1(g, ab, d, j):
        return rdma(
            ob_small(g, ab, j), ob_small(g, ab, j), g1_s.at[g, ab, d - 1], g1_r.at[g, ab, d - 1], second[ab](d)
        )

    def g2a(g, ab, k, j):
        return rdma(
            ob_big(g, ab, j), ob_big(g, ab, j),
            g2_s.at[g, 0, ab, k], g2_r.at[g, 0, ab, k], first[ab](HOP[k]),
        )

    def g2b(g, ab, k, j):
        ref = ob_big(g, ab, j, k)
        return rdma(ref, ref, g2_s.at[g, 1, ab, k], g2_r.at[g, 1, ab, k], first[ab](HOP[k]))

    def do_f(g):
        for k in (1, 2, 3):
            rdma(vx.at[g], rx.at[g, k], x_s.at[g], x_r.at[g, k], mate).wait_recv()
        for ab in range(2):
            acc = vx[g, ab].astype(F32)
            for k in (1, 2, 3):
                acc = acc + rx[g, k, ab].astype(F32)
            ob_small(g, ab, i2[ab])[...] = acc.astype(BF)
        for ab, d in PAIRS:
            g1(g, ab, d, i2[ab]).start()

    def do_g2a(g):
        for ab, d in PAIRS:
            g1(g, ab, d, (i2[ab] + 4 - d) % 4).wait_recv()
        for ab, k in BOTH:
            g2a(g, ab, k, i1[ab]).start()

    def do_g2b(g):
        for ab, k in BOTH:
            g2a(g, ab, k, (i1[ab] + HOP[1 - k]) % 4).wait_recv()
        for ab, k in BOTH:
            g2b(g, ab, k, (i1[ab] + HOP[1 - k]) % 4).start()

    def do_out(g):
        for ab, k in BOTH:
            g2b(g, ab, k, (i1[ab] + 2) % 4).wait_recv()

        def body(i, _):
            r = pl.ds(al(g * 128 + i * 16, 16), 16)
            gw_ref[r, :] = ob[r, :].astype(F32)
            return 0

        lax.fori_loop(0, 8, body, 0)

    def arrive(s):
        wx(arrival[s]).wait_recv()
        relay(s, c).start()

    def unit_body(u, _):
        slot = u % 2
        xu, par, _q = unit(u)
        relay(u, o).wait_recv()

        @pl.when(u < 7)
        def _():
            for cpy in uv_copies(u + 1):
                cpy.start()

        gs[...] = dot_nt(d_v[...], wbuf[u].reshape(256, WID)).astype(BF)

        for cpy in uv_copies(u):
            cpy.wait()

        for cls in range(2):
            row = bias_ref[pl.ds(4 * xu + 2 * cls + par, 1), :]
            bb[cls] = jnp.broadcast_to(row, (128, 128)).T
        gwacc[...] = jnp.zeros_like(gwacc)
        bacc[...] = jnp.zeros_like(bacc)
        gacc[...] = jnp.zeros_like(gacc)
        sacc[...] = jnp.zeros_like(sacc)

        def block(n, _):
            r = pl.ds(al(n * 128, 128), 128)
            for cls in range(2):
                grp = 4 * xu + 2 * cls + par
                ln = pl.ds(cls * 128, 128)
                gain = gain_ref[pl.ds(grp, 1), :]
                shift = shift_ref[pl.ds(grp, 1), :]
                gated = gelu_value(vb[slot, r, ln].astype(F32))
                cen = gated - lane_mean(gated)
                inv = lax.rsqrt(lane_mean(cen * cen) + EPS)
                scaled = cen * inv
                gv_ref[0, r, cols(u, cls)] = scaled.astype(BF)
                sinv[u, r, ln] = jnp.broadcast_to(inv, (128, 128)).astype(BF)
                nb = (scaled * gain + shift).astype(BF)
                upper, u_slope = gelu_pair(ub[slot, r, ln].astype(F32))
                cot = gs[r, ln].astype(F32)
                dm = cot * upper
                dmb = dm.astype(BF)
                bacc[cls] += dm
                mixed = dot_nn(wl[grp], nb) + bb[cls]
                dn = dot_nn(wlt[grp], dmb)
                gwacc[cls] += dot_nt(dmb, nb)
                gt[pl.ds(cls * 128, 128), r] = (upper * mixed).T.astype(BF)
                gu_ref[0, r, cols(u, cls)] = (cot * mixed * u_slope).astype(BF)
                prod = dn * scaled
                gacc[cls] += jnp.sum(prod.reshape(16, 8, 128), axis=0)
                sacc[cls] += jnp.sum(dn.reshape(16, 8, 128), axis=0)
                sdn[u, r, ln] = dn.astype(BF)
            return 0

        lax.fori_loop(0, 8, block, 0, unroll=4)

        for lag, act in ((5, do_x), (4, do_s2b), (3, do_s2a), (2, do_s1b), (1, do_ts)):

            @pl.when(u >= lag)
            def _(lag=lag, act=act):
                act(u - lag)

        pb[slot, :, :, pl.ds(0, WID)] = dot_nn(gt[...], d_v[...]).astype(BF).reshape(2, 128, WID)
        for cls in range(2):
            grp = 4 * xu + 2 * cls + par
            pb[slot, cls, :, pl.ds(WID, 128)] = jnp.where(tri, gwacc[cls], 0.0).astype(BF)
            st[0, pl.ds(grp, 1), :] = jnp.sum(bacc[cls].T, axis=0, keepdims=True)
            st[1, pl.ds(grp, 1), :] = jnp.sum(gacc[cls], axis=0, keepdims=True)
            st[2, pl.ds(grp, 1), :] = jnp.sum(sacc[cls], axis=0, keepdims=True)
        ps(u).start()

        @pl.when(u == 1)
        def _():
            arrive(2)
            wx(4).start()
            arrive(3)
            wx(5).start()

        @pl.when(u == 3)
        def _():
            arrive(4)
            arrive(5)

        @pl.when(u == 5)
        def _():
            arrive(6)
            arrive(7)

        return 0

    lax.fori_loop(0, 8, unit_body, 0)

    def v_copies(u):
        return uv_copies(u)[2:]

    def finish(u):
        slot = u % 2
        xu, par, _ = unit(u)
        for cpy in v_copies(u):
            cpy.wait()
        if u < 7:
            for cpy in v_copies(u + 1):
                cpy.start()

        def block(n, _):
            r = pl.ds(al(n * 128, 128), 128)
            for cls in range(2):
                ln = pl.ds(cls * 128, 128)
                gain = gain_ref[pl.ds(4 * xu + 2 * cls + par, 1), :]
                slope = gelu_slope(vb[slot, r, ln].astype(F32))
                scaled = gv_ref[0, r, cols(u, cls)].astype(F32)
                e = sdn[u, r, ln].astype(F32) * gain
                m1 = lane_mean(e)
                m2 = lane_mean(e * scaled)
                gv_ref[0, r, cols(u, cls)] = (
                    (e - m1 - scaled * m2) * (slope * sinv[u, r, ln].astype(F32))
                ).astype(BF)
            return 0

        lax.fori_loop(0, 8, block, 0, unroll=4)

    for cpy in v_copies(0):
        cpy.start()

    def stat_sum(src, parts, dst):
        acc = src[...]
        for part in parts:
            acc = acc + part[...]
        dst[...] = acc

    t0 = rdma(st, rs0, t_s.at[0, 0], t_r.at[0, 0], mate)
    t0.start()

    def tstage(k, d, src, f):
        return rdma(src, rs1.at[k, d - 1], t_s.at[k + 1, d - 1], t_r.at[k + 1, d - 1], f(d))

    def cz(d, j):
        return rdma(qc.at[pl.ds(2 * j, 2)], rc2.at[d - 1], c_s.at[1, d - 1], c_r.at[1, d - 1], pz(d))

    def cx(d):
        return rdma(qd, rc3.at[d - 1], c_s.at[2, d - 1], c_r.at[2, d - 1], px(d))

    def cgz(d, j):
        ref = cg.at[pl.ds(2 * j, 2), pl.ds(al(32 * y, 32), 32)]
        return rdma(ref, ref, c_s.at[3, d - 1], c_r.at[3, d - 1], pz(d))

    def cga(k, j):
        ref = cg.at[:, pl.ds(al(32 * j, 32), 32)]
        return rdma(ref, ref, c_s.at[4, k], c_r.at[4, k], py(HOP[k]))

    def cgb(k, j):
        ref = cg.at[pl.ds(4 * k, 4), pl.ds(al(32 * j, 32), 32)]
        return rdma(ref, ref, c_s.at[0, k], c_r.at[0, k], py(HOP[k]))

    DS = (1, 2, 3)

    def pipe(n):
        for lag, act in ((5, do_x), (4, do_s2b), (3, do_s2a), (2, do_s1b), (1, do_ts)):
            if 0 <= n - lag <= 7:
                act(n - lag)

    def stat_step(k, f, g):
        for d in DS:
            tstage(k, d, st2.at[k], f).wait()
        if k < 2:
            stat_sum(st2.at[k], [rs1.at[k, i] for i in range(3)], st2.at[k + 1])
            for d in DS:
                tstage(k + 1, d, st2.at[k + 1], g).start()

    finish(0)
    pipe(8)
    t0.wait()
    stat_sum(st, [rs0], st2.at[0])
    for d in DS:
        tstage(0, d, st2.at[0], py).start()
    finish(1)
    pipe(9)
    stat_step(0, py, pz)
    finish(2)
    pipe(10)
    for d in DS:
        cz(d, (z + d) % 4).start()
    stat_step(1, pz, px)
    finish(3)
    pipe(11)
    for d in DS:
        cz(d, (z + d) % 4).wait()
    acc = qc[pl.ds(2 * z, 2)].astype(F32)
    for k in range(3):
        acc = acc + rc2[k].astype(F32)
    qd[...] = acc.astype(BF)
    for d in DS:
        cx(d).start()
    finish(4)
    pipe(12)
    do_f(0)
    for d in DS:
        cx(d).wait()
    acc = qd[...].astype(F32)
    for k in range(3):
        acc = acc + rc3[k].astype(F32)
    cg[pl.ds(2 * z, 2), pl.ds(al(32 * y, 32), 32), :] = acc.astype(BF)
    for d in DS:
        cgz(d, z).start()
    stat_step(2, px, None)
    tot = st2[2]
    for k in range(3):
        tot = tot + rs1[2, k]
    stat_ref[...] = tot
    finish(5)
    do_f(1)
    do_g2a(0)
    for d in DS:
        cgz(d, (z + 4 - d) % 4).wait_recv()
    for k in range(2):
        cga(k, y).start()
    finish(6)
    do_g2a(1)
    do_g2b(0)
    for k in range(2):
        cga(k, (y + HOP[1 - k]) % 4).wait_recv()
    for k in range(2):
        cgb(k, (y + HOP[1 - k]) % 4).start()
    finish(7)
    do_g2b(1)
    for k in range(2):
        cgb(k, (y + 2) % 4).wait_recv()
    swap = rdma(cg, cp, c_s.at[5, 0], c_r.at[5, 0], mate)
    swap.start()
    do_out(0)

    def gm_body(src, cls):
        def body(i, _):
            gm_ref[(i // 2) * 4 + 2 * cls + i % 2] = src[i].astype(F32)
            return 0

        lax.fori_loop(0, 8, body, 0)

    gm_body(cg, c)
    do_out(1)
    swap.wait()
    gm_body(cp, o)

    for k in range(6):
        wx(k).wait_send()
    for s in range(8):
        relay(s, c).wait_send()
    for u in range(2, 8):
        xs(u).wait_send()
    for g in range(2):
        for ab, d in PAIRS:
            g1(g, ab, d, i2[ab]).wait_send()
        for ab, k in BOTH:
            g2a(g, ab, k, i1[ab]).wait_send()
            g2b(g, ab, k, (i1[ab] + HOP[1 - k]) % 4).wait_send()
    for d in DS:
        cgz(d, z).wait_send()
    for k in range(2):
        cga(k, y).wait_send()
        cgb(k, (y + HOP[1 - k]) % 4).wait_send()


def place(gu, gv, gw, gm, st, o_gu, o_gv, o_gw, o_gm, o_b, o_g, o_s, sem):
    moves = [(gu, o_gu), (gv, o_gv), (gw, o_gw), (gm, o_gm), (st.at[0], o_b), (st.at[1], o_g), (st.at[2], o_s)]
    cps = [pltpu.make_async_copy(a, b, sem.at[i]) for i, (a, b) in enumerate(moves)]
    for cpy in cps:
        cpy.start()
    for cpy in cps:
        cpy.wait()


def on_device(u_pre, v_pre, d_out, w_mix, mix_bias, norm_gain, norm_shift, w_out):
    hbm = pl.BlockSpec(memory_space=pltpu.HBM)
    vm = pl.BlockSpec(memory_space=pltpu.VMEM)
    V = pltpu.VMEM
    DMA = pltpu.SemaphoreType.DMA
    scratch = [
        V((1024, WID), BF), V((8, 2, 128, WID), BF),
        V((2, 1024, 256), BF), V((2, 1024, 256), BF),
        V((1024, 256), BF), V((256, 1024), BF),
        V((2, 2, 128, EXT), BF), V((2, 128, EXT), BF), V((4, 128, EXT), BF),
        V((8, 2, 2, 16, 1152), BF), V((8, 2, 2, 32, 1152), BF), V((4, 2, 32, 1024), BF),
        V((8, 2, 2, 16, 256), BF), V((8, 2, 2, 32, 256), BF),
        V((8, 2, 32, 256), BF), V((2, 4, 2, 32, 256), BF), V((256, WID), BF),
        V((8, 32, 128), BF), V((3, 2, 32, 128), BF),
        V((2, 32, 128), BF), V((3, 2, 32, 128), BF), V((8, 128, 128), BF), V((8, 128, 128), BF),
        V((3, 16, 128), F32), V((3, 3, 16, 128), F32), V((3, 16, 128), F32), V((3, 3, 3, 16, 128), F32),
        V((16, 128), F32), V((16, 128), F32), V((16, 128), F32),
        V((16, 128, 128), BF), V((16, 128, 128), BF), V((2, 128, 128), F32),
        V((2, 128, 128), F32), V((2, 128, 128), F32), V((2, 8, 128), F32), V((2, 8, 128), F32),
        V((8, 1024, 256), BF), V((8, 1024, 256), BF),
        DMA((10,)), DMA((2, 2, 2)), DMA((6,)), DMA((6,)), DMA((8,)), DMA((8,)),
        DMA((2,)), DMA((8,)), DMA((4, 2, 2, 2)), DMA((8, 2, 2, 2)), DMA((4, 2, 2, 2)), DMA((8, 2, 2, 2)),
        DMA((8,)), DMA((2, 4)), DMA((2, 2, 3)), DMA((2, 2, 3)), DMA((2, 2, 2, 2)), DMA((2, 2, 2, 2)),
        DMA((6, 3)), DMA((6, 3)), DMA((4, 3)), DMA((4, 3)),
    ]
    outs = pl.pallas_call(
        kernel,
        out_shape=(
            jax.ShapeDtypeStruct(u_pre.shape, BF),
            jax.ShapeDtypeStruct(v_pre.shape, BF),
            jax.ShapeDtypeStruct((256, WID), F32),
            jax.ShapeDtypeStruct((16, 128, 128), F32),
            jax.ShapeDtypeStruct((3, 16, 128), F32),
        ),
        in_specs=[hbm] * 8,
        out_specs=(vm, vm, vm, vm, vm),
        scratch_shapes=scratch,
        compiler_params=pltpu.CompilerParams(
            collective_id=0, has_side_effects=True, vmem_limit_bytes=39 * 1024 * 1024
        ),
    )(u_pre, v_pre, d_out, w_mix, mix_bias, norm_gain, norm_shift, w_out)
    anyspace = pl.BlockSpec(memory_space=pl.ANY)
    small = jax.ShapeDtypeStruct((16, 128), F32)
    return pl.pallas_call(
        place,
        out_shape=(
            jax.ShapeDtypeStruct(u_pre.shape, BF),
            jax.ShapeDtypeStruct(v_pre.shape, BF),
            jax.ShapeDtypeStruct((256, WID), F32),
            jax.ShapeDtypeStruct((16, 128, 128), F32),
            small, small, small,
        ),
        in_specs=[anyspace] * 5,
        out_specs=(hbm,) * 7,
        scratch_shapes=[DMA((7,))],
        compiler_params=pltpu.CompilerParams(vmem_limit_bytes=512 * 1024),
    )(*outs)


def solution(mesh):
    return jax.shard_map(
        on_device,
        mesh=mesh,
        in_specs=(
            P("dp", "sp", None), P("dp", "sp", None), P("dp", "sp", None),
            P(), P(), P(), P(), P("dp", None),
        ),
        out_specs=(P("dp", "sp", None), P("dp", "sp", None), P("dp", None), P(), P(), P(), P()),
        check_vma=False,
    )
```

```python
import functools

import jax
import jax.numpy as jnp
from jax import lax
from jax.experimental import pallas as pl
from jax.experimental.pallas import tpu as pltpu
from jax.sharding import PartitionSpec as P

EPS = 1e-05
C0 = 0.7978845608028654
C1 = 0.044715
F32 = jnp.float32
BF = jnp.bfloat16
MESH = pl.DeviceIdType.MESH
WID = 2048
EXT = WID + 128


def rdma(src, dst, ssem, rsem, dev):
    return pltpu.make_async_remote_copy(
        src_ref=src, dst_ref=dst, send_sem=ssem, recv_sem=rsem, device_id=dev, device_id_type=MESH
    )


def al(v, m):
    return pl.multiple_of(v, m)


def gelu_pair(a):
    a2 = a * a
    th = jnp.tanh(a * (C0 + (C0 * C1) * a2))
    s = 0.5 + 0.5 * th
    g = a * s
    slope = s + g * (1.0 - s) * (2.0 * C0 + (6.0 * C0 * C1) * a2)
    return g, slope


def gelu_value(a):
    return a * (0.5 + 0.5 * jnp.tanh(a * (C0 + (C0 * C1) * (a * a))))


def gelu_slope(a):
    return gelu_pair(a)[1]


def lane_mean(a):
    return jnp.sum(a, axis=-1, keepdims=True) * (1.0 / 128.0)


def dot_nn(a, b):
    return lax.dot_general(a, b, (((1,), (0,)), ((), ())), preferred_element_type=F32)


def dot_nt(a, b):
    return lax.dot_general(a, b, (((1,), (1,)), ((), ())), preferred_element_type=F32)


def kernel(
    u_hbm, v_hbm, d_hbm, wm_hbm, bias_hbm, gain_hbm, shift_hbm, w_hbm,
    gu_ref, gv_ref, gw_ref, gm_ref, stat_ref,
    d_v, wbuf, ub, vb, gs, gt, pb, pr, tb, ra, rb, q, rc, rd, vx, rx, ob,
    qc, rc2, qd, rc3, cg, cp,
    st, st2, rs0, rs1, bias_ref, gain_ref, shift_ref, wl, wlt, bb, gwacc, bacc, gacc, sacc,
    sinv, sdn,
    ld_s, uv_s, wsend, wrecv, wrel_s, wrel_r,
    ps_s, ps_r, s1_s, s1_r, s2_s, s2_r, x_s, x_r, g1_s, g1_r, g2_s, g2_r,
    c_s, c_r, t_s, t_r,
):
    sp = lax.axis_index("sp")
    dp = lax.axis_index("dp")
    z, y = sp // 4, sp % 4
    x, c = dp // 2, dp % 2
    o = 1 - c

    def dev(x_, y_, z_, c_):
        return (z_ * 4 + y_, x_ * 2 + c_)

    def px(d):
        return dev((x + d) % 4, y, z, c)

    def py(d):
        return dev(x, (y + d) % 4, z, c)

    def pz(d):
        return dev(x, y, (z + d) % 4, c)

    mate = dev(x, y, z, o)
    first = (py, pz)
    second = (pz, py)
    i1 = (y, z)
    i2 = (z, y)

    own = [
        pltpu.make_async_copy(w_hbm.at[pl.ds(g * 128, 128)], wbuf.at[g, c], ld_s.at[g]) for g in range(2)
    ]
    dcp = [
        pltpu.make_async_copy(
            d_hbm.at[0, pl.ds(i * 256, 256)], d_v.at[pl.ds(i * 256, 256)], ld_s.at[2 + i]
        )
        for i in range(4)
    ]
    for cpy in own:
        cpy.start()
    params = [
        pltpu.make_async_copy(a, b, ld_s.at[6 + i])
        for i, (a, b) in enumerate(
            ((wm_hbm, wl), (bias_hbm, bias_ref), (gain_hbm, gain_ref), (shift_hbm, shift_ref))
        )
    ]
    for cpy in params:
        cpy.start()
    for cpy in dcp:
        cpy.start()

    def unit(u, cls):
        par = u % 2
        quad = u // 2
        xu = (x + jnp.where(cls == 0, 4 - quad, quad)) % 4
        return xu, par, quad

    def group(u, cls):
        xu, par, _ = unit(u, cls)
        return 4 * xu + 2 * cls + par

    def cols(u, cls):
        return pl.ds(al(group(u, cls) * 128, 128), 128)

    def uv_copies(u):
        slot = u % 2
        res = []
        for k, (hbm, buf) in enumerate(((u_hbm, ub), (v_hbm, vb))):
            for cls in range(2):
                res.append(
                    pltpu.make_async_copy(
                        hbm.at[0, :, cols(u, cls)],
                        buf.at[slot, :, pl.ds(cls * 128, 128)],
                        uv_s.at[slot, k, cls],
                    )
                )
        return res

    for cpy in uv_copies(0):
        cpy.start()

    barrier = pltpu.get_barrier_semaphore()
    for peer in [mate] + [f(d) for f in (px, py, pz) for d in (1, 2, 3)]:
        pl.semaphore_signal(barrier, inc=1, device_id=peer, device_id_type=MESH)
    pl.semaphore_wait(barrier, 10)

    def wx(k):
        return rdma(wbuf.at[k, c], wbuf.at[k + 2, c], wsend.at[k], wrecv.at[k], px(1 + 2 * c))

    def relay(s, k):
        return rdma(wbuf.at[s, k], wbuf.at[s, k], wrel_s.at[s], wrel_r.at[s], mate)

    for cpy in own:
        cpy.wait()
    relay(0, c).start()
    relay(1, c).start()
    for k in range(2):
        wx(k).start()

    tri = lax.broadcasted_iota(jnp.int32, (128, 128), 0) >= lax.broadcasted_iota(jnp.int32, (128, 128), 1)

    def prep(g, _):
        w = jnp.where(tri, wl[g].astype(F32), 0.0)
        wl[g] = w.astype(BF)
        wlt[g] = w.T.astype(BF)
        return 0

    for cpy in params:
        cpy.wait()
    lax.fori_loop(0, 16, prep, 0)
    for cpy in dcp:
        cpy.wait()

    def ps(u):
        return rdma(pb.at[u % 2, o], pr.at[u % 2], ps_s.at[u % 2], ps_r.at[u], mate)

    WAB = (1152, 1024)
    OFF = (0, 1152)

    def rows(j, half=None):
        if half is None:
            return pl.ds(al(32 * j, 32), 32)
        return pl.ds(al(32 * j + 16 * half, 16), 16)

    def lanes(j):
        return pl.ds(al(256 * j, 256), 256)

    HOP = (1, 3)

    def s1a(u, ab, k):
        w = WAB[ab]
        return rdma(
            tb.at[u % 4, rows((i1[ab] + 2) % 4, k), pl.ds(OFF[ab], w)],
            ra.at[u, ab, k, :, pl.ds(0, w)],
            s1_s.at[u % 4, 0, ab, k], s1_r.at[u, 0, ab, k], first[ab](HOP[k]),
        )

    def s1b(u, ab, k):
        w = WAB[ab]
        return rdma(
            tb.at[u % 4, rows((i1[ab] + HOP[k]) % 4), pl.ds(OFF[ab], w)],
            rb.at[u, ab, k, :, pl.ds(0, w)],
            s1_s.at[u % 4, 1, ab, k], s1_r.at[u, 1, ab, k], first[ab](HOP[k]),
        )

    def s2a(u, ab, k):
        return rdma(
            q.at[u % 4, ab, pl.ds(16 * k, 16), lanes((i2[ab] + 2) % 4)],
            rc.at[u, ab, k],
            s2_s.at[u % 4, 0, ab, k], s2_r.at[u, 0, ab, k], second[ab](HOP[k]),
        )

    def s2b(u, ab, k):
        return rdma(
            q.at[u % 4, ab, :, lanes((i2[ab] + HOP[k]) % 4)],
            rd.at[u, ab, k],
            s2_s.at[u % 4, 1, ab, k], s2_r.at[u, 1, ab, k], second[ab](HOP[k]),
        )

    def xs(u):
        xu, par, quad = unit(u, c)
        return rdma(vx.at[u], rx.at[par, quad], x_s.at[u], x_r.at[par, quad], dev(xu, y, z, c))

    PAIRS = [(ab, d) for ab in range(2) for d in (1, 2, 3)]
    BOTH = [(ab, k) for ab in range(2) for k in range(2)]

    def do_ts(u):
        ps(u).wait()
        slot = u % 4

        def body(i, _):
            r = pl.ds(al(i * 16, 16), 16)
            for src, dst, w in ((0, 0, 1024), (WID, 1024, 128), (1024, 1152, 1024)):
                tb[slot, r, pl.ds(dst, w)] = pb[u % 2, c, r, pl.ds(src, w)] + pr[u % 2, r, pl.ds(src, w)]
            return 0

        lax.fori_loop(0, 8, body, 0)
        for ab, k in BOTH:
            s1a(u, ab, k).start()

    def do_s1b(u):
        slot = u % 4
        for ab, k in BOTH:
            s1a(u, ab, k).wait_recv()
        for ab, k in BOTH:
            r, ln = rows((i1[ab] + HOP[k]) % 4, k), pl.ds(OFF[ab], WAB[ab])
            tb[slot, r, ln] = tb[slot, r, ln] + ra[u, ab, k, :, pl.ds(0, WAB[ab])]
        for ab, k in BOTH:
            s1b(u, ab, k).start()

    def do_s2a(u):
        slot = u % 4
        xu, par, _ = unit(u, c)
        for ab, k in BOTH:
            s1a(u, ab, k).wait_send()
            s1b(u, ab, k).wait()
        for ab in range(2):
            for h in range(2):
                hs = pl.ds(16 * h, 16)

                def total(a, w):
                    acc = tb[slot, rows(i1[ab], h), pl.ds(OFF[ab] + a, w)].astype(F32)
                    for k in range(2):
                        acc = acc + rb[u, ab, k, hs, pl.ds(a, w)].astype(F32)
                    return acc.astype(BF)

                q[slot, ab, hs, :] = total(0, 1024)
                if ab == 0:
                    qc[xu * 2 + par, hs, :] = total(1024, 128)
        for ab, k in BOTH:
            s2a(u, ab, k).start()

    def do_s2b(u):
        slot = u % 4
        for ab, k in BOTH:
            s2a(u, ab, k).wait_recv()
        for ab, k in BOTH:
            hs, ln = pl.ds(16 * k, 16), lanes((i2[ab] + HOP[k]) % 4)
            q[slot, ab, hs, ln] = q[slot, ab, hs, ln] + rc[u, ab, k]
        for ab, k in BOTH:
            s2b(u, ab, k).start()

    def do_x(u):
        slot = u % 4
        for ab, k in BOTH:
            s2a(u, ab, k).wait_send()
            s2b(u, ab, k).wait()
        for ab in range(2):
            acc = q[slot, ab, :, lanes(i2[ab])].astype(F32)
            for k in range(2):
                acc = acc + rd[u, ab, k].astype(F32)
            vx[u, ab] = acc.astype(BF)

        @pl.when(u >= 2)
        def _():
            xs(u).start()

    def ob_small(g, ab, j):
        return ob.at[
            pl.ds(al(g * 128 + 32 * i1[ab], 32), 32), pl.ds(al(1024 * ab + 256 * j, 256), 256)
        ]

    def ob_big(g, ab, j, half=None):
        r = pl.ds(al(g * 128 + 32 * j, 32), 32)
        if half is not None:
            r = pl.ds(al(g * 128 + 32 * j + 16 * half, 16), 16)
        return ob.at[r, pl.ds(1024 * ab, 1024)]

    def g1(g, ab, d, j):
        return rdma(
            ob_small(g, ab, j), ob_small(g, ab, j), g1_s.at[g, ab, d - 1], g1_r.at[g, ab, d - 1], second[ab](d)
        )

    def g2a(g, ab, k, j):
        return rdma(
            ob_big(g, ab, j), ob_big(g, ab, j),
            g2_s.at[g, 0, ab, k], g2_r.at[g, 0, ab, k], first[ab](HOP[k]),
        )

    def g2b(g, ab, k, j):
        ref = ob_big(g, ab, j, k)
        return rdma(ref, ref, g2_s.at[g, 1, ab, k], g2_r.at[g, 1, ab, k], first[ab](HOP[k]))

    def do_f(g):
        for k in (1, 2, 3):
            rdma(vx.at[g], rx.at[g, k], x_s.at[g], x_r.at[g, k], mate).wait_recv()
        for ab in range(2):
            acc = vx[g, ab].astype(F32)
            for k in (1, 2, 3):
                acc = acc + rx[g, k, ab].astype(F32)
            ob_small(g, ab, i2[ab])[...] = acc.astype(BF)
        for ab, d in PAIRS:
            g1(g, ab, d, i2[ab]).start()

    def do_g2a(g):
        for ab, d in PAIRS:
            g1(g, ab, d, (i2[ab] + 4 - d) % 4).wait_recv()
        for ab, k in BOTH:
            g2a(g, ab, k, i1[ab]).start()

    def do_g2b(g):
        for ab, k in BOTH:
            g2a(g, ab, k, (i1[ab] + HOP[1 - k]) % 4).wait_recv()
        for ab, k in BOTH:
            g2b(g, ab, k, (i1[ab] + HOP[1 - k]) % 4).start()

    def do_out(g):
        for ab, k in BOTH:
            g2b(g, ab, k, (i1[ab] + 2) % 4).wait_recv()

        def body(i, _):
            r = pl.ds(al(g * 128 + i * 16, 16), 16)
            gw_ref[r, :] = ob[r, :].astype(F32)
            return 0

        lax.fori_loop(0, 8, body, 0)

    def arrive(s):
        wx(s - 2).wait_recv()
        relay(s, c).start()

        @pl.when(s < 6)
        def _():
            wx(s).start()

    def unit_body(u, _):
        slot = u % 2
        relay(u, o).wait_recv()

        @pl.when(u < 7)
        def _():
            for cpy in uv_copies(u + 1):
                cpy.start()

        gs[...] = dot_nt(d_v[...], wbuf[u].reshape(256, WID)).astype(BF)

        @pl.when((u >= 1) & (u < 7))
        def _():
            arrive(u + 1)


        for cpy in uv_copies(u):
            cpy.wait()

        for cls in range(2):
            row = bias_ref[pl.ds(group(u, cls), 1), :]
            bb[cls] = jnp.broadcast_to(row, (128, 128)).T
        gwacc[...] = jnp.zeros_like(gwacc)
        bacc[...] = jnp.zeros_like(bacc)
        gacc[...] = jnp.zeros_like(gacc)
        sacc[...] = jnp.zeros_like(sacc)

        def block(n, _):
            r = pl.ds(al(n * 128, 128), 128)
            for cls in range(2):
                grp = group(u, cls)
                ln = pl.ds(cls * 128, 128)
                gain = gain_ref[pl.ds(grp, 1), :]
                shift = shift_ref[pl.ds(grp, 1), :]
                gated = gelu_value(vb[slot, r, ln].astype(F32))
                cen = gated - lane_mean(gated)
                inv = lax.rsqrt(lane_mean(cen * cen) + EPS)
                scaled = cen * inv
                gv_ref[0, r, cols(u, cls)] = scaled.astype(BF)
                sinv[u, r, ln] = jnp.broadcast_to(inv, (128, 128)).astype(BF)
                nb = (scaled * gain + shift).astype(BF)
                upper = gelu_value(ub[slot, r, ln].astype(F32))
                cot = gs[r, ln].astype(F32)
                dm = cot * upper
                dmb = dm.astype(BF)
                bacc[cls] += dm
                mixed = dot_nn(wl[grp], nb) + bb[cls]
                dn = dot_nn(wlt[grp], dmb)
                gwacc[cls] += dot_nt(dmb, nb)
                gt[pl.ds(cls * 128, 128), r] = (upper * mixed).T.astype(BF)
                gu_ref[0, r, cols(u, cls)] = (cot * mixed).astype(BF)
                prod = dn * scaled
                gacc[cls] += jnp.sum(prod.reshape(16, 8, 128), axis=0)
                sacc[cls] += jnp.sum(dn.reshape(16, 8, 128), axis=0)
                sdn[u, r, ln] = dn.astype(BF)
            return 0

        lax.fori_loop(0, 8, block, 0, unroll=4)

        for lag, act in ((5, do_x), (4, do_s2b), (3, do_s2a), (2, do_s1b), (1, do_ts)):

            @pl.when(u >= lag)
            def _(lag=lag, act=act):
                act(u - lag)

        pb[slot, :, :, pl.ds(0, WID)] = dot_nn(gt[...], d_v[...]).astype(BF).reshape(2, 128, WID)
        for cls in range(2):
            grp = group(u, cls)
            pb[slot, cls, :, pl.ds(WID, 128)] = jnp.where(tri, gwacc[cls], 0.0).astype(BF)
            st[0, pl.ds(grp, 1), :] = jnp.sum(bacc[cls].T, axis=0, keepdims=True)
            st[1, pl.ds(grp, 1), :] = jnp.sum(gacc[cls], axis=0, keepdims=True)
            st[2, pl.ds(grp, 1), :] = jnp.sum(sacc[cls], axis=0, keepdims=True)
        ps(u).start()

        return 0

    lax.fori_loop(0, 8, unit_body, 0)

    def v_copies(u):
        return uv_copies(u)

    def finish(u):
        slot = u % 2
        for cpy in v_copies(u):
            cpy.wait()
        if u < 7:
            for cpy in v_copies(u + 1):
                cpy.start()

        def block(n, _):
            r = pl.ds(al(n * 128, 128), 128)
            for cls in range(2):
                ln = pl.ds(cls * 128, 128)
                gain = gain_ref[pl.ds(group(u, cls), 1), :]
                cl = cols(u, cls)
                gu_ref[0, r, cl] = (
                    gu_ref[0, r, cl].astype(F32) * gelu_slope(ub[slot, r, ln].astype(F32))
                ).astype(BF)
                slope = gelu_slope(vb[slot, r, ln].astype(F32))
                scaled = gv_ref[0, r, cols(u, cls)].astype(F32)
                e = sdn[u, r, ln].astype(F32) * gain
                m1 = lane_mean(e)
                m2 = lane_mean(e * scaled)
                gv_ref[0, r, cols(u, cls)] = (
                    (e - m1 - scaled * m2) * (slope * sinv[u, r, ln].astype(F32))
                ).astype(BF)
            return 0

        lax.fori_loop(0, 8, block, 0, unroll=4)

    for cpy in v_copies(0):
        cpy.start()

    def stat_sum(src, parts, dst):
        acc = src[...]
        for part in parts:
            acc = acc + part[...]
        dst[...] = acc

    t0 = rdma(st, rs0, t_s.at[0, 0], t_r.at[0, 0], mate)
    t0.start()

    def tstage(k, d, src, f):
        return rdma(src, rs1.at[k, d - 1], t_s.at[k + 1, d - 1], t_r.at[k + 1, d - 1], f(d))

    def cz(d, j):
        return rdma(qc.at[pl.ds(2 * j, 2)], rc2.at[d - 1], c_s.at[1, d - 1], c_r.at[1, d - 1], pz(d))

    def cx(d):
        return rdma(qd, rc3.at[d - 1], c_s.at[2, d - 1], c_r.at[2, d - 1], px(d))

    def cgz(d, j):
        ref = cg.at[pl.ds(2 * j, 2), pl.ds(al(32 * y, 32), 32)]
        return rdma(ref, ref, c_s.at[3, d - 1], c_r.at[3, d - 1], pz(d))

    def cga(k, j):
        ref = cg.at[:, pl.ds(al(32 * j, 32), 32)]
        return rdma(ref, ref, c_s.at[4, k], c_r.at[4, k], py(HOP[k]))

    def cgb(k, j):
        ref = cg.at[pl.ds(4 * k, 4), pl.ds(al(32 * j, 32), 32)]
        return rdma(ref, ref, c_s.at[0, k], c_r.at[0, k], py(HOP[k]))

    DS = (1, 2, 3)

    def pipe(n):
        for lag, act in ((5, do_x), (4, do_s2b), (3, do_s2a), (2, do_s1b), (1, do_ts)):
            if 0 <= n - lag <= 7:
                act(n - lag)

    def stat_step(k, f, g):
        for d in DS:
            tstage(k, d, st2.at[k], f).wait()
        if k < 2:
            stat_sum(st2.at[k], [rs1.at[k, i] for i in range(3)], st2.at[k + 1])
            for d in DS:
                tstage(k + 1, d, st2.at[k + 1], g).start()

    finish(0)
    pipe(8)
    t0.wait()
    stat_sum(st, [rs0], st2.at[0])
    for d in DS:
        tstage(0, d, st2.at[0], py).start()
    finish(1)
    pipe(9)
    stat_step(0, py, pz)
    finish(2)
    pipe(10)
    for d in DS:
        cz(d, (z + d) % 4).start()
    stat_step(1, pz, px)
    finish(3)
    pipe(11)
    for d in DS:
        cz(d, (z + d) % 4).wait()
    acc = qc[pl.ds(2 * z, 2)].astype(F32)
    for k in range(3):
        acc = acc + rc2[k].astype(F32)
    qd[...] = acc.astype(BF)
    for d in DS:
        cx(d).start()
    finish(4)
    pipe(12)
    do_f(0)
    for d in DS:
        cx(d).wait()
    acc = qd[...].astype(F32)
    for k in range(3):
        acc = acc + rc3[k].astype(F32)
    cg[pl.ds(2 * z, 2), pl.ds(al(32 * y, 32), 32), :] = acc.astype(BF)
    for d in DS:
        cgz(d, z).start()
    stat_step(2, px, None)
    tot = st2[2]
    for k in range(3):
        tot = tot + rs1[2, k]
    stat_ref[...] = tot
    finish(5)
    do_f(1)
    do_g2a(0)
    for d in DS:
        cgz(d, (z + 4 - d) % 4).wait_recv()
    for k in range(2):
        cga(k, y).start()
    finish(6)
    do_g2a(1)
    do_g2b(0)
    for k in range(2):
        cga(k, (y + HOP[1 - k]) % 4).wait_recv()
    for k in range(2):
        cgb(k, (y + HOP[1 - k]) % 4).start()
    finish(7)
    do_g2b(1)
    for k in range(2):
        cgb(k, (y + 2) % 4).wait_recv()
    swap = rdma(cg, cp, c_s.at[5, 0], c_r.at[5, 0], mate)
    swap.start()
    do_out(0)

    def gm_body(src, cls):
        def body(i, _):
            gm_ref[(i // 2) * 4 + 2 * cls + i % 2] = src[i].astype(F32)
            return 0

        lax.fori_loop(0, 8, body, 0)

    gm_body(cg, c)
    do_out(1)
    swap.wait()
    gm_body(cp, o)

    for k in range(6):
        wx(k).wait_send()
    for s in range(8):
        relay(s, c).wait_send()
    for u in range(2, 8):
        xs(u).wait_send()
    for g in range(2):
        for ab, d in PAIRS:
            g1(g, ab, d, i2[ab]).wait_send()
        for ab, k in BOTH:
            g2a(g, ab, k, i1[ab]).wait_send()
            g2b(g, ab, k, (i1[ab] + HOP[1 - k]) % 4).wait_send()
    for d in DS:
        cgz(d, z).wait_send()
    for k in range(2):
        cga(k, y).wait_send()
        cgb(k, (y + HOP[1 - k]) % 4).wait_send()


def place(gu, gv, gw, gm, st, o_gu, o_gv, o_gw, o_gm, o_b, o_g, o_s, sem):
    moves = [(gu, o_gu), (gv, o_gv), (gw, o_gw), (gm, o_gm), (st.at[0], o_b), (st.at[1], o_g), (st.at[2], o_s)]
    cps = [pltpu.make_async_copy(a, b, sem.at[i]) for i, (a, b) in enumerate(moves)]
    for cpy in cps:
        cpy.start()
    for cpy in cps:
        cpy.wait()


def on_device(u_pre, v_pre, d_out, w_mix, mix_bias, norm_gain, norm_shift, w_out):
    hbm = pl.BlockSpec(memory_space=pltpu.HBM)
    vm = pl.BlockSpec(memory_space=pltpu.VMEM)
    V = pltpu.VMEM
    DMA = pltpu.SemaphoreType.DMA
    scratch = [
        V((1024, WID), BF), V((8, 2, 128, WID), BF),
        V((2, 1024, 256), BF), V((2, 1024, 256), BF),
        V((1024, 256), BF), V((256, 1024), BF),
        V((2, 2, 128, EXT), BF), V((2, 128, EXT), BF), V((4, 128, EXT), BF),
        V((8, 2, 2, 16, 1152), BF), V((8, 2, 2, 32, 1152), BF), V((4, 2, 32, 1024), BF),
        V((8, 2, 2, 16, 256), BF), V((8, 2, 2, 32, 256), BF),
        V((8, 2, 32, 256), BF), V((2, 4, 2, 32, 256), BF), V((256, WID), BF),
        V((8, 32, 128), BF), V((3, 2, 32, 128), BF),
        V((2, 32, 128), BF), V((3, 2, 32, 128), BF), V((8, 128, 128), BF), V((8, 128, 128), BF),
        V((3, 16, 128), F32), V((3, 3, 16, 128), F32), V((3, 16, 128), F32), V((3, 3, 3, 16, 128), F32),
        V((16, 128), F32), V((16, 128), F32), V((16, 128), F32),
        V((16, 128, 128), BF), V((16, 128, 128), BF), V((2, 128, 128), F32),
        V((2, 128, 128), F32), V((2, 128, 128), F32), V((2, 8, 128), F32), V((2, 8, 128), F32),
        V((8, 1024, 256), BF), V((8, 1024, 256), BF),
        DMA((10,)), DMA((2, 2, 2)), DMA((6,)), DMA((6,)), DMA((8,)), DMA((8,)),
        DMA((2,)), DMA((8,)), DMA((4, 2, 2, 2)), DMA((8, 2, 2, 2)), DMA((4, 2, 2, 2)), DMA((8, 2, 2, 2)),
        DMA((8,)), DMA((2, 4)), DMA((2, 2, 3)), DMA((2, 2, 3)), DMA((2, 2, 2, 2)), DMA((2, 2, 2, 2)),
        DMA((6, 3)), DMA((6, 3)), DMA((4, 3)), DMA((4, 3)),
    ]
    outs = pl.pallas_call(
        kernel,
        out_shape=(
            jax.ShapeDtypeStruct(u_pre.shape, BF),
            jax.ShapeDtypeStruct(v_pre.shape, BF),
            jax.ShapeDtypeStruct((256, WID), F32),
            jax.ShapeDtypeStruct((16, 128, 128), F32),
            jax.ShapeDtypeStruct((3, 16, 128), F32),
        ),
        in_specs=[hbm] * 8,
        out_specs=(vm, vm, vm, vm, vm),
        scratch_shapes=scratch,
        compiler_params=pltpu.CompilerParams(
            collective_id=0, has_side_effects=True, vmem_limit_bytes=39 * 1024 * 1024
        ),
    )(u_pre, v_pre, d_out, w_mix, mix_bias, norm_gain, norm_shift, w_out)
    anyspace = pl.BlockSpec(memory_space=pl.ANY)
    small = jax.ShapeDtypeStruct((16, 128), F32)
    return pl.pallas_call(
        place,
        out_shape=(
            jax.ShapeDtypeStruct(u_pre.shape, BF),
            jax.ShapeDtypeStruct(v_pre.shape, BF),
            jax.ShapeDtypeStruct((256, WID), F32),
            jax.ShapeDtypeStruct((16, 128, 128), F32),
            small, small, small,
        ),
        in_specs=[anyspace] * 5,
        out_specs=(hbm,) * 7,
        scratch_shapes=[DMA((7,))],
        compiler_params=pltpu.CompilerParams(vmem_limit_bytes=512 * 1024),
    )(*outs)


def solution(mesh):
    return jax.shard_map(
        on_device,
        mesh=mesh,
        in_specs=(
            P("dp", "sp", None), P("dp", "sp", None), P("dp", "sp", None),
            P(), P(), P(), P(), P("dp", None),
        ),
        out_specs=(P("dp", "sp", None), P("dp", "sp", None), P("dp", None), P(), P(), P(), P()),
        check_vma=False,
    )
```

```python
import functools

import jax
import jax.numpy as jnp
from jax import lax
from jax.experimental import pallas as pl
from jax.experimental.pallas import tpu as pltpu
from jax.sharding import PartitionSpec as P

EPS = 1e-05
C0 = 0.7978845608028654
C1 = 0.044715
F32 = jnp.float32
BF = jnp.bfloat16
MESH = pl.DeviceIdType.MESH
WID = 2048
EXT = WID + 128


def rdma(src, dst, ssem, rsem, dev):
    return pltpu.make_async_remote_copy(
        src_ref=src, dst_ref=dst, send_sem=ssem, recv_sem=rsem, device_id=dev, device_id_type=MESH
    )


def al(v, m):
    return pl.multiple_of(v, m)


def gelu_pair(a):
    a2 = a * a
    th = jnp.tanh(a * (C0 + (C0 * C1) * a2))
    s = 0.5 + 0.5 * th
    g = a * s
    slope = s + g * (1.0 - s) * (2.0 * C0 + (6.0 * C0 * C1) * a2)
    return g, slope


def gelu_value(a):
    return a * (0.5 + 0.5 * jnp.tanh(a * (C0 + (C0 * C1) * (a * a))))


def gelu_slope(a):
    return gelu_pair(a)[1]


def lane_mean(a):
    return jnp.sum(a, axis=-1, keepdims=True) * (1.0 / 128.0)


def dot_nn(a, b):
    return lax.dot_general(a, b, (((1,), (0,)), ((), ())), preferred_element_type=F32)


def dot_nt(a, b):
    return lax.dot_general(a, b, (((1,), (1,)), ((), ())), preferred_element_type=F32)


def kernel(
    u_hbm, v_hbm, d_hbm, wm_hbm, bias_hbm, gain_hbm, shift_hbm, w_hbm,
    gu_ref, gv_ref, gw_ref, gm_ref, stat_ref,
    d_v, wbuf, ub, vb, gs, gt, pb, pr, tb, ct, ra, rb, rcy, q, rc, vx, rx, ob,
    qc, rc2, qd, rc3, cg, cp,
    st, st2, rs0, rs1, bias_ref, gain_ref, shift_ref, wl, wlt, bb, gwacc, bacc, gacc, sacc,
    sinv, sdn,
    ld_s, uv_s, wsend, wrecv, wrel_s, wrel_r,
    ps_s, ps_r, s1_s, s1_r, s2_s, s2_r, x_s, x_r, g1_s, g1_r, g2_s, g2_r,
    c_s, c_r, t_s, t_r, cy_s, cy_r,
):
    sp = lax.axis_index("sp")
    dp = lax.axis_index("dp")
    z, y = sp // 4, sp % 4
    x, c = dp // 2, dp % 2
    o = 1 - c

    def dev(x_, y_, z_, c_):
        return (z_ * 4 + y_, x_ * 2 + c_)

    def px(d):
        return dev((x + d) % 4, y, z, c)

    def py(d):
        return dev(x, (y + d) % 4, z, c)

    def pz(d):
        return dev(x, y, (z + d) % 4, c)

    mate = dev(x, y, z, o)
    first = (py, pz)
    second = (pz, py)
    i1 = (y, z)
    i2 = (z, y)

    own = [
        pltpu.make_async_copy(w_hbm.at[pl.ds(g * 128, 128)], wbuf.at[g, c], ld_s.at[g]) for g in range(2)
    ]
    dcp = [
        pltpu.make_async_copy(
            d_hbm.at[0, pl.ds(i * 256, 256)], d_v.at[pl.ds(i * 256, 256)], ld_s.at[2 + i]
        )
        for i in range(4)
    ]
    for cpy in own:
        cpy.start()
    params = [
        pltpu.make_async_copy(a, b, ld_s.at[6 + i])
        for i, (a, b) in enumerate(
            ((wm_hbm, wl), (bias_hbm, bias_ref), (gain_hbm, gain_ref), (shift_hbm, shift_ref))
        )
    ]
    for cpy in params:
        cpy.start()
    for cpy in dcp:
        cpy.start()

    def unit(u, cls):
        par = u % 2
        quad = u // 2
        xu = (x + jnp.where(cls == 0, 4 - quad, quad)) % 4
        return xu, par, quad

    def group(u, cls):
        xu, par, _ = unit(u, cls)
        return 4 * xu + 2 * cls + par

    def cols(u, cls):
        return pl.ds(al(group(u, cls) * 128, 128), 128)

    def uv_copies(u):
        slot = u % 2
        res = []
        for k, (hbm, buf) in enumerate(((u_hbm, ub), (v_hbm, vb))):
            for cls in range(2):
                res.append(
                    pltpu.make_async_copy(
                        hbm.at[0, :, cols(u, cls)],
                        buf.at[slot, :, pl.ds(cls * 128, 128)],
                        uv_s.at[slot, k, cls],
                    )
                )
        return res

    for cpy in uv_copies(0):
        cpy.start()

    barrier = pltpu.get_barrier_semaphore()
    for peer in [mate] + [f(d) for f in (px, py, pz) for d in (1, 2, 3)]:
        pl.semaphore_signal(barrier, inc=1, device_id=peer, device_id_type=MESH)
    pl.semaphore_wait(barrier, 10)

    def wx(k):
        return rdma(wbuf.at[k, c], wbuf.at[k + 2, c], wsend.at[k], wrecv.at[k], px(1 + 2 * c))

    def relay(s, k):
        return rdma(wbuf.at[s, k], wbuf.at[s, k], wrel_s.at[s], wrel_r.at[s], mate)

    for cpy in own:
        cpy.wait()
    relay(0, c).start()
    relay(1, c).start()
    for k in range(2):
        wx(k).start()

    tri = lax.broadcasted_iota(jnp.int32, (128, 128), 0) >= lax.broadcasted_iota(jnp.int32, (128, 128), 1)

    def prep(g, _):
        w = jnp.where(tri, wl[g].astype(F32), 0.0)
        wl[g] = w.astype(BF)
        wlt[g] = w.T.astype(BF)
        return 0

    for cpy in params:
        cpy.wait()
    lax.fori_loop(0, 16, prep, 0)
    for cpy in dcp:
        cpy.wait()

    def ps(u):
        return rdma(pb.at[u % 2, o], pr.at[u % 2], ps_s.at[u % 2], ps_r.at[u], mate)

    WAB = (1024, 1024)
    OFF = (0, 1024)

    def rows(j, half=None):
        if half is None:
            return pl.ds(al(32 * j, 32), 32)
        return pl.ds(al(32 * j + 16 * half, 16), 16)

    def lanes(j):
        return pl.ds(al(256 * j, 256), 256)

    HOP = (1, 3)

    def s1a(u, ab, k):
        w = WAB[ab]
        return rdma(
            tb.at[u % 4, rows((i1[ab] + 2) % 4, k), pl.ds(OFF[ab], w)],
            ra.at[u, ab, k, :, pl.ds(0, w)],
            s1_s.at[u % 4, 0, ab, k], s1_r.at[u, 0, ab, k], first[ab](HOP[k]),
        )

    def s1b(u, ab, k):
        w = WAB[ab]
        return rdma(
            tb.at[u % 4, rows((i1[ab] + HOP[k]) % 4), pl.ds(OFF[ab], w)],
            rb.at[u, ab, k, :, pl.ds(0, w)],
            s1_s.at[u % 4, 1, ab, k], s1_r.at[u, 1, ab, k], first[ab](HOP[k]),
        )

    def s2(u, ab, d):
        return rdma(
            q.at[u % 4, ab, :, lanes((i2[ab] + d) % 4)], rc.at[u, ab, d - 1],
            s2_s.at[u % 4, ab, d - 1], s2_r.at[u, ab, d - 1], second[ab](d),
        )

    def cy(u, d):
        return rdma(
            ct.at[u % 4, rows((y + d) % 4)], rcy.at[u, d - 1],
            cy_s.at[u % 4, d - 1], cy_r.at[u, d - 1], py(d),
        )

    def xs(u):
        xu, par, quad = unit(u, c)
        return rdma(vx.at[u], rx.at[par, quad], x_s.at[u], x_r.at[par, quad], dev(xu, y, z, c))

    DS = (1, 2, 3)
    PAIRS = [(ab, d) for ab in range(2) for d in (1, 2, 3)]
    BOTH = [(ab, k) for ab in range(2) for k in range(2)]

    def do_ts(u):
        ps(u).wait()
        slot = u % 4

        def body(i, _):
            r = pl.ds(al(i * 16, 16), 16)
            w, e = pl.ds(0, WID), pl.ds(WID, 128)
            tb[slot, r, :] = pb[u % 2, c, r, w] + pr[u % 2, r, w]
            ct[slot, r, :] = pb[u % 2, c, r, e] + pr[u % 2, r, e]
            return 0

        lax.fori_loop(0, 8, body, 0)
        for ab, k in BOTH:
            s1a(u, ab, k).start()
        for d in DS:
            cy(u, d).start()

    def do_s1b(u):
        slot = u % 4
        for ab, k in BOTH:
            s1a(u, ab, k).wait_recv()
        for ab, k in BOTH:
            r, ln = rows((i1[ab] + HOP[k]) % 4, k), pl.ds(OFF[ab], WAB[ab])
            tb[slot, r, ln] = tb[slot, r, ln] + ra[u, ab, k, :, pl.ds(0, WAB[ab])]
        for ab, k in BOTH:
            s1b(u, ab, k).start()
        for d in DS:
            cy(u, d).wait()
        xu, par, _ = unit(u, c)
        acc = ct[slot, rows(y), :].astype(F32)
        for k in range(3):
            acc = acc + rcy[u, k].astype(F32)
        qc[xu * 2 + par] = acc.astype(BF)

    def do_s2a(u):
        slot = u % 4
        for ab, k in BOTH:
            s1a(u, ab, k).wait_send()
            s1b(u, ab, k).wait()
        for ab in range(2):
            for h in range(2):
                hs = pl.ds(16 * h, 16)

                def total(a, w):
                    acc = tb[slot, rows(i1[ab], h), pl.ds(OFF[ab] + a, w)].astype(F32)
                    for k in range(2):
                        acc = acc + rb[u, ab, k, hs, pl.ds(a, w)].astype(F32)
                    return acc.astype(BF)

                q[slot, ab, hs, :] = total(0, 1024)
        for ab, d in PAIRS:
            s2(u, ab, d).start()

    def do_x(u):
        slot = u % 4
        for ab, d in PAIRS:
            s2(u, ab, d).wait()
        for ab in range(2):
            acc = q[slot, ab, :, lanes(i2[ab])].astype(F32)
            for k in range(3):
                acc = acc + rc[u, ab, k].astype(F32)
            vx[u, ab] = acc.astype(BF)

        @pl.when(u >= 2)
        def _():
            xs(u).start()

    def ob_small(g, ab, j):
        return ob.at[
            pl.ds(al(g * 128 + 32 * i1[ab], 32), 32), pl.ds(al(1024 * ab + 256 * j, 256), 256)
        ]

    def ob_big(g, ab, j, half=None):
        r = pl.ds(al(g * 128 + 32 * j, 32), 32)
        if half is not None:
            r = pl.ds(al(g * 128 + 32 * j + 16 * half, 16), 16)
        return ob.at[r, pl.ds(1024 * ab, 1024)]

    def g1(g, ab, d, j):
        return rdma(
            ob_small(g, ab, j), ob_small(g, ab, j), g1_s.at[g, ab, d - 1], g1_r.at[g, ab, d - 1], second[ab](d)
        )

    def g2a(g, ab, k, j):
        return rdma(
            ob_big(g, ab, j), ob_big(g, ab, j),
            g2_s.at[g, 0, ab, k], g2_r.at[g, 0, ab, k], first[ab](HOP[k]),
        )

    def g2b(g, ab, k, j):
        ref = ob_big(g, ab, j, k)
        return rdma(ref, ref, g2_s.at[g, 1, ab, k], g2_r.at[g, 1, ab, k], first[ab](HOP[k]))

    def do_f(g):
        for k in (1, 2, 3):
            rdma(vx.at[g], rx.at[g, k], x_s.at[g], x_r.at[g, k], mate).wait_recv()
        for ab in range(2):
            acc = vx[g, ab].astype(F32)
            for k in (1, 2, 3):
                acc = acc + rx[g, k, ab].astype(F32)
            ob_small(g, ab, i2[ab])[...] = acc.astype(BF)
        for ab, d in PAIRS:
            g1(g, ab, d, i2[ab]).start()

    def do_g2a(g):
        for ab, d in PAIRS:
            g1(g, ab, d, (i2[ab] + 4 - d) % 4).wait_recv()
        for ab, k in BOTH:
            g2a(g, ab, k, i1[ab]).start()

    def do_g2b(g):
        for ab, k in BOTH:
            g2a(g, ab, k, (i1[ab] + HOP[1 - k]) % 4).wait_recv()
        for ab, k in BOTH:
            g2b(g, ab, k, (i1[ab] + HOP[1 - k]) % 4).start()

    def do_out(g):
        for ab, k in BOTH:
            g2b(g, ab, k, (i1[ab] + 2) % 4).wait_recv()

        def body(i, _):
            r = pl.ds(al(g * 128 + i * 16, 16), 16)
            gw_ref[r, :] = ob[r, :].astype(F32)
            return 0

        lax.fori_loop(0, 8, body, 0)

    def arrive(s):
        wx(s - 2).wait_recv()
        relay(s, c).start()

        @pl.when(s < 6)
        def _():
            wx(s).start()

    def unit_body(u, _):
        slot = u % 2
        relay(u, o).wait_recv()

        @pl.when(u < 7)
        def _():
            for cpy in uv_copies(u + 1):
                cpy.start()

        gs[...] = dot_nt(d_v[...], wbuf[u].reshape(256, WID)).astype(BF)

        @pl.when((u >= 1) & (u < 7))
        def _():
            arrive(u + 1)


        for cpy in uv_copies(u):
            cpy.wait()

        for cls in range(2):
            row = bias_ref[pl.ds(group(u, cls), 1), :]
            bb[cls] = jnp.broadcast_to(row, (128, 128)).T
        gwacc[...] = jnp.zeros_like(gwacc)
        bacc[...] = jnp.zeros_like(bacc)
        gacc[...] = jnp.zeros_like(gacc)
        sacc[...] = jnp.zeros_like(sacc)

        def block(n, _):
            r = pl.ds(al(n * 128, 128), 128)
            for cls in range(2):
                grp = group(u, cls)
                ln = pl.ds(cls * 128, 128)
                gain = gain_ref[pl.ds(grp, 1), :]
                shift = shift_ref[pl.ds(grp, 1), :]
                gated = gelu_value(vb[slot, r, ln].astype(F32))
                cen = gated - lane_mean(gated)
                inv = lax.rsqrt(lane_mean(cen * cen) + EPS)
                scaled = cen * inv
                gv_ref[0, r, cols(u, cls)] = scaled.astype(BF)
                sinv[u, r, ln] = jnp.broadcast_to(inv, (128, 128)).astype(BF)
                nb = (scaled * gain + shift).astype(BF)
                upper = gelu_value(ub[slot, r, ln].astype(F32))
                cot = gs[r, ln].astype(F32)
                dm = cot * upper
                dmb = dm.astype(BF)
                bacc[cls] += dm
                mixed = dot_nn(wl[grp], nb) + bb[cls]
                dn = dot_nn(wlt[grp], dmb)
                gwacc[cls] += dot_nt(dmb, nb)
                gt[pl.ds(cls * 128, 128), r] = (upper * mixed).T.astype(BF)
                gu_ref[0, r, cols(u, cls)] = (cot * mixed).astype(BF)
                prod = dn * scaled
                gacc[cls] += jnp.sum(prod.reshape(16, 8, 128), axis=0)
                sacc[cls] += jnp.sum(dn.reshape(16, 8, 128), axis=0)
                sdn[u, r, ln] = dn.astype(BF)
            return 0

        lax.fori_loop(0, 8, block, 0, unroll=4)

        for lag, act in ((4, do_x), (3, do_s2a), (2, do_s1b), (1, do_ts)):

            @pl.when(u >= lag)
            def _(lag=lag, act=act):
                act(u - lag)

        pb[slot, :, :, pl.ds(0, WID)] = dot_nn(gt[...], d_v[...]).astype(BF).reshape(2, 128, WID)
        for cls in range(2):
            grp = group(u, cls)
            pb[slot, cls, :, pl.ds(WID, 128)] = jnp.where(tri, gwacc[cls], 0.0).astype(BF)
            st[0, pl.ds(grp, 1), :] = jnp.sum(bacc[cls].T, axis=0, keepdims=True)
            st[1, pl.ds(grp, 1), :] = jnp.sum(gacc[cls], axis=0, keepdims=True)
            st[2, pl.ds(grp, 1), :] = jnp.sum(sacc[cls], axis=0, keepdims=True)
        ps(u).start()

        return 0

    lax.fori_loop(0, 8, unit_body, 0)

    def v_copies(u):
        return uv_copies(u)

    def finish(u):
        slot = u % 2
        for cpy in v_copies(u):
            cpy.wait()
        if u < 7:
            for cpy in v_copies(u + 1):
                cpy.start()

        def block(n, _):
            r = pl.ds(al(n * 128, 128), 128)
            for cls in range(2):
                ln = pl.ds(cls * 128, 128)
                gain = gain_ref[pl.ds(group(u, cls), 1), :]
                cl = cols(u, cls)
                gu_ref[0, r, cl] = (
                    gu_ref[0, r, cl].astype(F32) * gelu_slope(ub[slot, r, ln].astype(F32))
                ).astype(BF)
                slope = gelu_slope(vb[slot, r, ln].astype(F32))
                scaled = gv_ref[0, r, cols(u, cls)].astype(F32)
                e = sdn[u, r, ln].astype(F32) * gain
                m1 = lane_mean(e)
                m2 = lane_mean(e * scaled)
                gv_ref[0, r, cols(u, cls)] = (
                    (e - m1 - scaled * m2) * (slope * sinv[u, r, ln].astype(F32))
                ).astype(BF)
            return 0

        lax.fori_loop(0, 8, block, 0, unroll=4)

    for cpy in v_copies(0):
        cpy.start()

    def stat_sum(src, parts, dst):
        acc = src[...]
        for part in parts:
            acc = acc + part[...]
        dst[...] = acc

    t0 = rdma(st, rs0, t_s.at[0, 0], t_r.at[0, 0], mate)
    t0.start()

    def tstage(k, d, src, f):
        return rdma(src, rs1.at[k, d - 1], t_s.at[k + 1, d - 1], t_r.at[k + 1, d - 1], f(d))

    def cz(d, j):
        return rdma(qc.at[pl.ds(2 * j, 2)], rc2.at[d - 1], c_s.at[1, d - 1], c_r.at[1, d - 1], pz(d))

    def cx(d):
        return rdma(qd, rc3.at[d - 1], c_s.at[2, d - 1], c_r.at[2, d - 1], px(d))

    def cgz(d, j):
        ref = cg.at[pl.ds(2 * j, 2), pl.ds(al(32 * y, 32), 32)]
        return rdma(ref, ref, c_s.at[3, d - 1], c_r.at[3, d - 1], pz(d))

    def cga(k, j):
        ref = cg.at[:, pl.ds(al(32 * j, 32), 32)]
        return rdma(ref, ref, c_s.at[4, k], c_r.at[4, k], py(HOP[k]))

    def cgb(k, j):
        ref = cg.at[pl.ds(4 * k, 4), pl.ds(al(32 * j, 32), 32)]
        return rdma(ref, ref, c_s.at[0, k], c_r.at[0, k], py(HOP[k]))


    def pipe(n):
        for lag, act in ((4, do_x), (3, do_s2a), (2, do_s1b), (1, do_ts)):
            if 0 <= n - lag <= 7:
                act(n - lag)

    def stat_step(k, f, g):
        for d in DS:
            tstage(k, d, st2.at[k], f).wait()
        if k < 2:
            stat_sum(st2.at[k], [rs1.at[k, i] for i in range(3)], st2.at[k + 1])
            for d in DS:
                tstage(k + 1, d, st2.at[k + 1], g).start()

    finish(0)
    pipe(8)
    t0.wait()
    stat_sum(st, [rs0], st2.at[0])
    for d in DS:
        tstage(0, d, st2.at[0], py).start()
    finish(1)
    pipe(9)
    for d in DS:
        cz(d, (z + d) % 4).start()
    stat_step(0, py, pz)
    finish(2)
    pipe(10)
    for d in DS:
        cz(d, (z + d) % 4).wait()
    acc = qc[pl.ds(2 * z, 2)].astype(F32)
    for k in range(3):
        acc = acc + rc2[k].astype(F32)
    qd[...] = acc.astype(BF)
    for d in DS:
        cx(d).start()
    stat_step(1, pz, px)
    finish(3)
    pipe(11)
    do_f(0)
    for d in DS:
        cx(d).wait()
    acc = qd[...].astype(F32)
    for k in range(3):
        acc = acc + rc3[k].astype(F32)
    cg[pl.ds(2 * z, 2), pl.ds(al(32 * y, 32), 32), :] = acc.astype(BF)
    for d in DS:
        cgz(d, z).start()
    stat_step(2, px, None)
    tot = st2[2]
    for k in range(3):
        tot = tot + rs1[2, k]
    stat_ref[...] = tot
    finish(4)
    do_f(1)
    do_g2a(0)
    for d in DS:
        cgz(d, (z + 4 - d) % 4).wait_recv()
    for k in range(2):
        cga(k, y).start()
    finish(5)
    do_g2a(1)
    do_g2b(0)
    for k in range(2):
        cga(k, (y + HOP[1 - k]) % 4).wait_recv()
    for k in range(2):
        cgb(k, (y + HOP[1 - k]) % 4).start()
    finish(6)
    do_g2b(1)
    for k in range(2):
        cgb(k, (y + 2) % 4).wait_recv()
    swap = rdma(cg, cp, c_s.at[5, 0], c_r.at[5, 0], mate)
    swap.start()
    finish(7)
    do_out(0)

    def gm_body(src, cls):
        def body(i, _):
            gm_ref[(i // 2) * 4 + 2 * cls + i % 2] = src[i].astype(F32)
            return 0

        lax.fori_loop(0, 8, body, 0)

    gm_body(cg, c)
    do_out(1)
    swap.wait()
    gm_body(cp, o)

    for k in range(6):
        wx(k).wait_send()
    for s in range(8):
        relay(s, c).wait_send()
    for u in range(2, 8):
        xs(u).wait_send()
    for g in range(2):
        for ab, d in PAIRS:
            g1(g, ab, d, i2[ab]).wait_send()
        for ab, k in BOTH:
            g2a(g, ab, k, i1[ab]).wait_send()
            g2b(g, ab, k, (i1[ab] + HOP[1 - k]) % 4).wait_send()
    for d in DS:
        cgz(d, z).wait_send()
    for k in range(2):
        cga(k, y).wait_send()
        cgb(k, (y + HOP[1 - k]) % 4).wait_send()


def place(gu, gv, gw, gm, st, o_gu, o_gv, o_gw, o_gm, o_b, o_g, o_s, sem):
    moves = [(gu, o_gu), (gv, o_gv), (gw, o_gw), (gm, o_gm), (st.at[0], o_b), (st.at[1], o_g), (st.at[2], o_s)]
    cps = [pltpu.make_async_copy(a, b, sem.at[i]) for i, (a, b) in enumerate(moves)]
    for cpy in cps:
        cpy.start()
    for cpy in cps:
        cpy.wait()


def on_device(u_pre, v_pre, d_out, w_mix, mix_bias, norm_gain, norm_shift, w_out):
    hbm = pl.BlockSpec(memory_space=pltpu.HBM)
    vm = pl.BlockSpec(memory_space=pltpu.VMEM)
    V = pltpu.VMEM
    DMA = pltpu.SemaphoreType.DMA
    scratch = [
        V((1024, WID), BF), V((8, 2, 128, WID), BF),
        V((2, 1024, 256), BF), V((2, 1024, 256), BF),
        V((1024, 256), BF), V((256, 1024), BF),
        V((2, 2, 128, EXT), BF), V((2, 128, EXT), BF), V((4, 128, WID), BF), V((4, 128, 128), BF),
        V((8, 2, 2, 16, 1024), BF), V((8, 2, 2, 32, 1024), BF), V((8, 3, 32, 128), BF), V((4, 2, 32, 1024), BF),
        V((8, 2, 3, 32, 256), BF),
        V((8, 2, 32, 256), BF), V((2, 4, 2, 32, 256), BF), V((256, WID), BF),
        V((8, 32, 128), BF), V((3, 2, 32, 128), BF),
        V((2, 32, 128), BF), V((3, 2, 32, 128), BF), V((8, 128, 128), BF), V((8, 128, 128), BF),
        V((3, 16, 128), F32), V((3, 3, 16, 128), F32), V((3, 16, 128), F32), V((3, 3, 3, 16, 128), F32),
        V((16, 128), F32), V((16, 128), F32), V((16, 128), F32),
        V((16, 128, 128), BF), V((16, 128, 128), BF), V((2, 128, 128), F32),
        V((2, 128, 128), F32), V((2, 128, 128), F32), V((2, 8, 128), F32), V((2, 8, 128), F32),
        V((8, 1024, 256), BF), V((8, 1024, 256), BF),
        DMA((10,)), DMA((2, 2, 2)), DMA((6,)), DMA((6,)), DMA((8,)), DMA((8,)),
        DMA((2,)), DMA((8,)), DMA((4, 2, 2, 2)), DMA((8, 2, 2, 2)), DMA((4, 2, 3)), DMA((8, 2, 3)),
        DMA((8,)), DMA((2, 4)), DMA((2, 2, 3)), DMA((2, 2, 3)), DMA((2, 2, 2, 2)), DMA((2, 2, 2, 2)),
        DMA((6, 3)), DMA((6, 3)), DMA((4, 3)), DMA((4, 3)), DMA((4, 3)), DMA((8, 3)),
    ]
    outs = pl.pallas_call(
        kernel,
        out_shape=(
            jax.ShapeDtypeStruct(u_pre.shape, BF),
            jax.ShapeDtypeStruct(v_pre.shape, BF),
            jax.ShapeDtypeStruct((256, WID), F32),
            jax.ShapeDtypeStruct((16, 128, 128), F32),
            jax.ShapeDtypeStruct((3, 16, 128), F32),
        ),
        in_specs=[hbm] * 8,
        out_specs=(vm, vm, vm, vm, vm),
        scratch_shapes=scratch,
        compiler_params=pltpu.CompilerParams(
            collective_id=0, has_side_effects=True, vmem_limit_bytes=39 * 1024 * 1024
        ),
    )(u_pre, v_pre, d_out, w_mix, mix_bias, norm_gain, norm_shift, w_out)
    anyspace = pl.BlockSpec(memory_space=pl.ANY)
    small = jax.ShapeDtypeStruct((16, 128), F32)
    return pl.pallas_call(
        place,
        out_shape=(
            jax.ShapeDtypeStruct(u_pre.shape, BF),
            jax.ShapeDtypeStruct(v_pre.shape, BF),
            jax.ShapeDtypeStruct((256, WID), F32),
            jax.ShapeDtypeStruct((16, 128, 128), F32),
            small, small, small,
        ),
        in_specs=[anyspace] * 5,
        out_specs=(hbm,) * 7,
        scratch_shapes=[DMA((7,))],
        compiler_params=pltpu.CompilerParams(vmem_limit_bytes=512 * 1024),
    )(*outs)


def solution(mesh):
    return jax.shard_map(
        on_device,
        mesh=mesh,
        in_specs=(
            P("dp", "sp", None), P("dp", "sp", None), P("dp", "sp", None),
            P(), P(), P(), P(), P("dp", None),
        ),
        out_specs=(P("dp", "sp", None), P("dp", "sp", None), P("dp", None), P(), P(), P(), P()),
        check_vma=False,
    )
```

```python
import functools

import jax
import jax.numpy as jnp
from jax import lax
from jax.experimental import pallas as pl
from jax.experimental.pallas import tpu as pltpu
from jax.sharding import PartitionSpec as P

EPS = 1e-05
C0 = 0.7978845608028654
C1 = 0.044715
F32 = jnp.float32
BF = jnp.bfloat16
MESH = pl.DeviceIdType.MESH
WID = 2048
EXT = WID + 128


def rdma(src, dst, ssem, rsem, dev):
    return pltpu.make_async_remote_copy(
        src_ref=src, dst_ref=dst, send_sem=ssem, recv_sem=rsem, device_id=dev, device_id_type=MESH
    )


def al(v, m):
    return pl.multiple_of(v, m)


def gelu_pair(a):
    a2 = a * a
    th = jnp.tanh(a * (C0 + (C0 * C1) * a2))
    s = 0.5 + 0.5 * th
    g = a * s
    slope = s + g * (1.0 - s) * (2.0 * C0 + (6.0 * C0 * C1) * a2)
    return g, slope


def gelu_value(a):
    return a * (0.5 + 0.5 * jnp.tanh(a * (C0 + (C0 * C1) * (a * a))))


def gelu_slope(a):
    return gelu_pair(a)[1]


def lane_mean(a):
    return jnp.sum(a, axis=-1, keepdims=True) * (1.0 / 128.0)


def dot_nn(a, b):
    return lax.dot_general(a, b, (((1,), (0,)), ((), ())), preferred_element_type=F32)


def dot_nt(a, b):
    return lax.dot_general(a, b, (((1,), (1,)), ((), ())), preferred_element_type=F32)


def kernel(
    u_hbm, v_hbm, d_hbm, wm_hbm, bias_hbm, gain_hbm, shift_hbm, w_hbm,
    gu_ref, gv_ref, gw_ref, gm_ref, stat_ref,
    d_v, wbuf, ub, vb, gs, gt, pb, pr, tb, ct, ra, rb, rcy, q, rc, vx, rx, ob,
    qc, rc2, qd, rc3, cg, cp,
    st, st2, rs0, rs1, bias_ref, gain_ref, shift_ref, wl, wlt, bb, gwacc, bacc, gacc, sacc,
    sinv, sdn,
    ld_s, uv_s, wsend, wrecv, wrel_s, wrel_r,
    ps_s, ps_r, s1_s, s1_r, s2_s, s2_r, x_s, x_r, g1_s, g1_r, g2_s, g2_r,
    c_s, c_r, t_s, t_r, cy_s, cy_r,
):
    sp = lax.axis_index("sp")
    dp = lax.axis_index("dp")
    z, y = sp // 4, sp % 4
    x, c = dp // 2, dp % 2
    o = 1 - c

    def dev(x_, y_, z_, c_):
        return (z_ * 4 + y_, x_ * 2 + c_)

    def px(d):
        return dev((x + d) % 4, y, z, c)

    def py(d):
        return dev(x, (y + d) % 4, z, c)

    def pz(d):
        return dev(x, y, (z + d) % 4, c)

    mate = dev(x, y, z, o)
    first = (py, pz)
    second = (pz, py)
    i1 = (y, z)
    i2 = (z, y)

    own = [
        pltpu.make_async_copy(w_hbm.at[pl.ds(g * 128, 128)], wbuf.at[g, c], ld_s.at[g]) for g in range(2)
    ]
    dcp = [
        pltpu.make_async_copy(
            d_hbm.at[0, pl.ds(i * 256, 256)], d_v.at[pl.ds(i * 256, 256)], ld_s.at[2 + i]
        )
        for i in range(4)
    ]
    for cpy in own:
        cpy.start()
    params = [
        pltpu.make_async_copy(a, b, ld_s.at[6 + i])
        for i, (a, b) in enumerate(
            ((wm_hbm, wl), (bias_hbm, bias_ref), (gain_hbm, gain_ref), (shift_hbm, shift_ref))
        )
    ]
    for cpy in params:
        cpy.start()
    for cpy in dcp:
        cpy.start()

    def unit(u, cls):
        par = u % 2
        quad = u // 2
        xu = (x + jnp.where(cls == 0, 4 - quad, quad)) % 4
        return xu, par, quad

    def group(u, cls):
        xu, par, _ = unit(u, cls)
        return 4 * xu + 2 * cls + par

    def cols(u, cls):
        return pl.ds(al(group(u, cls) * 128, 128), 128)

    def uv_copies(u):
        slot = u % 2
        res = []
        for k, (hbm, buf) in enumerate(((u_hbm, ub), (v_hbm, vb))):
            for cls in range(2):
                res.append(
                    pltpu.make_async_copy(
                        hbm.at[0, :, cols(u, cls)],
                        buf.at[slot, :, pl.ds(cls * 128, 128)],
                        uv_s.at[slot, k, cls],
                    )
                )
        return res

    for cpy in uv_copies(0):
        cpy.start()

    barrier = pltpu.get_barrier_semaphore()
    for peer in [mate] + [f(d) for f in (px, py, pz) for d in (1, 2, 3)]:
        pl.semaphore_signal(barrier, inc=1, device_id=peer, device_id_type=MESH)
    pl.semaphore_wait(barrier, 10)

    def wx(k):
        return rdma(wbuf.at[k, c], wbuf.at[k + 2, c], wsend.at[k], wrecv.at[k], px(1 + 2 * c))

    def relay(s, k):
        return rdma(wbuf.at[s, k], wbuf.at[s, k], wrel_s.at[s], wrel_r.at[s], mate)

    for cpy in own:
        cpy.wait()
    relay(0, c).start()
    relay(1, c).start()
    for k in range(2):
        wx(k).start()

    tri = lax.broadcasted_iota(jnp.int32, (128, 128), 0) >= lax.broadcasted_iota(jnp.int32, (128, 128), 1)

    def prep(g, _):
        w = jnp.where(tri, wl[g].astype(F32), 0.0)
        wl[g] = w.astype(BF)
        wlt[g] = w.T.astype(BF)
        return 0

    for cpy in params:
        cpy.wait()
    lax.fori_loop(0, 16, prep, 0)
    for cpy in dcp:
        cpy.wait()

    def ps(u):
        return rdma(pb.at[u % 2, o], pr.at[u % 2], ps_s.at[u % 2], ps_r.at[u], mate)

    WAB = (1024, 1024)
    OFF = (0, 1024)

    def rows(j, half=None):
        if half is None:
            return pl.ds(al(32 * j, 32), 32)
        return pl.ds(al(32 * j + 16 * half, 16), 16)

    def lanes(j):
        return pl.ds(al(256 * j, 256), 256)

    HOP = (1, 3)

    def s1a(u, ab, k):
        w = WAB[ab]
        return rdma(
            tb.at[u % 4, rows((i1[ab] + 2) % 4, k), pl.ds(OFF[ab], w)],
            ra.at[u, ab, k, :, pl.ds(0, w)],
            s1_s.at[u % 4, 0, ab, k], s1_r.at[u, 0, ab, k], first[ab](HOP[k]),
        )

    def s1b(u, ab, k):
        w = WAB[ab]
        return rdma(
            tb.at[u % 4, rows((i1[ab] + HOP[k]) % 4), pl.ds(OFF[ab], w)],
            rb.at[u, ab, k, :, pl.ds(0, w)],
            s1_s.at[u % 4, 1, ab, k], s1_r.at[u, 1, ab, k], first[ab](HOP[k]),
        )

    def s2(u, ab, d):
        return rdma(
            q.at[u % 4, ab, :, lanes((i2[ab] + d) % 4)], rc.at[u, ab, d - 1],
            s2_s.at[u % 4, ab, d - 1], s2_r.at[u, ab, d - 1], second[ab](d),
        )

    def cy(u, d):
        return rdma(
            ct.at[u % 4, rows((y + d) % 4)], rcy.at[u, d - 1],
            cy_s.at[u % 4, d - 1], cy_r.at[u, d - 1], py(d),
        )

    def xs(u):
        xu, par, quad = unit(u, c)
        return rdma(vx.at[u], rx.at[par, quad], x_s.at[u], x_r.at[par, quad], dev(xu, y, z, c))

    DS = (1, 2, 3)
    PAIRS = [(ab, d) for ab in range(2) for d in (1, 2, 3)]
    BOTH = [(ab, k) for ab in range(2) for k in range(2)]

    def do_ts(u):
        ps(u).wait()
        slot = u % 4

        def body(i, _):
            r = pl.ds(al(i * 16, 16), 16)
            w, e = pl.ds(0, WID), pl.ds(WID, 128)
            tb[slot, r, :] = pb[u % 2, c, r, w] + pr[u % 2, r, w]
            ct[slot, r, :] = pb[u % 2, c, r, e] + pr[u % 2, r, e]
            return 0

        lax.fori_loop(0, 8, body, 0)
        for ab, k in BOTH:
            s1a(u, ab, k).start()
        for d in DS:
            cy(u, d).start()

    def do_s1b(u):
        slot = u % 4
        for ab, k in BOTH:
            s1a(u, ab, k).wait_recv()
        for ab, k in BOTH:
            r, ln = rows((i1[ab] + HOP[k]) % 4, k), pl.ds(OFF[ab], WAB[ab])
            tb[slot, r, ln] = tb[slot, r, ln] + ra[u, ab, k, :, pl.ds(0, WAB[ab])]
        for ab, k in BOTH:
            s1b(u, ab, k).start()
        for d in DS:
            cy(u, d).wait()
        xu, par, _ = unit(u, c)
        acc = ct[slot, rows(y), :].astype(F32)
        for k in range(3):
            acc = acc + rcy[u, k].astype(F32)
        qc[xu * 2 + par] = acc.astype(BF)

    def do_s2a(u):
        slot = u % 4
        for ab, k in BOTH:
            s1a(u, ab, k).wait_send()
            s1b(u, ab, k).wait()
        for ab in range(2):
            for h in range(2):
                hs = pl.ds(16 * h, 16)

                def total(a, w):
                    acc = tb[slot, rows(i1[ab], h), pl.ds(OFF[ab] + a, w)].astype(F32)
                    for k in range(2):
                        acc = acc + rb[u, ab, k, hs, pl.ds(a, w)].astype(F32)
                    return acc.astype(BF)

                q[slot, ab, hs, :] = total(0, 1024)
        for ab, d in PAIRS:
            s2(u, ab, d).start()

    def do_x(u):
        slot = u % 4
        for ab, d in PAIRS:
            s2(u, ab, d).wait()
        for ab in range(2):
            acc = q[slot, ab, :, lanes(i2[ab])].astype(F32)
            for k in range(3):
                acc = acc + rc[u, ab, k].astype(F32)
            vx[u, ab] = acc.astype(BF)

        @pl.when(u >= 2)
        def _():
            xs(u).start()

    def ob_small(g, ab, j):
        return ob.at[
            pl.ds(al(g * 128 + 32 * i1[ab], 32), 32), pl.ds(al(1024 * ab + 256 * j, 256), 256)
        ]

    def ob_big(g, ab, j, half=None):
        r = pl.ds(al(g * 128 + 32 * j, 32), 32)
        if half is not None:
            r = pl.ds(al(g * 128 + 32 * j + 16 * half, 16), 16)
        return ob.at[r, pl.ds(1024 * ab, 1024)]

    def g1(g, ab, d, j):
        return rdma(
            ob_small(g, ab, j), ob_small(g, ab, j), g1_s.at[g, ab, d - 1], g1_r.at[g, ab, d - 1], second[ab](d)
        )

    def g2a(g, ab, k, j):
        return rdma(
            ob_big(g, ab, j), ob_big(g, ab, j),
            g2_s.at[g, 0, ab, k], g2_r.at[g, 0, ab, k], first[ab](HOP[k]),
        )

    def g2b(g, ab, k, j):
        ref = ob_big(g, ab, j, k)
        return rdma(ref, ref, g2_s.at[g, 1, ab, k], g2_r.at[g, 1, ab, k], first[ab](HOP[k]))

    def do_f(g):
        for k in (1, 2, 3):
            rdma(vx.at[g], rx.at[g, k], x_s.at[g], x_r.at[g, k], mate).wait_recv()
        for ab in range(2):
            acc = vx[g, ab].astype(F32)
            for k in (1, 2, 3):
                acc = acc + rx[g, k, ab].astype(F32)
            ob_small(g, ab, i2[ab])[...] = acc.astype(BF)
        for ab, d in PAIRS:
            g1(g, ab, d, i2[ab]).start()

    def do_g2a(g):
        for ab, d in PAIRS:
            g1(g, ab, d, (i2[ab] + 4 - d) % 4).wait_recv()
        for ab, k in BOTH:
            g2a(g, ab, k, i1[ab]).start()

    def do_g2b(g):
        for ab, k in BOTH:
            g2a(g, ab, k, (i1[ab] + HOP[1 - k]) % 4).wait_recv()
        for ab, k in BOTH:
            g2b(g, ab, k, (i1[ab] + HOP[1 - k]) % 4).start()

    def do_out(g):
        for ab, k in BOTH:
            g2b(g, ab, k, (i1[ab] + 2) % 4).wait_recv()

        def body(i, _):
            r = pl.ds(al(g * 128 + i * 16, 16), 16)
            gw_ref[r, :] = ob[r, :].astype(F32)
            return 0

        lax.fori_loop(0, 8, body, 0)

    def arrive(s):
        wx(s - 2).wait_recv()
        relay(s, c).start()

        @pl.when(s < 6)
        def _():
            wx(s).start()

    def unit_body(u, _):
        slot = u % 2
        relay(u, o).wait_recv()

        @pl.when(u < 7)
        def _():
            for cpy in uv_copies(u + 1):
                cpy.start()

        gs[...] = dot_nt(d_v[...], wbuf[u].reshape(256, WID)).astype(BF)


        for cpy in uv_copies(u):
            cpy.wait()

        for cls in range(2):
            row = bias_ref[pl.ds(group(u, cls), 1), :]
            bb[cls] = jnp.broadcast_to(row, (128, 128)).T
        gwacc[...] = jnp.zeros_like(gwacc)
        bacc[...] = jnp.zeros_like(bacc)
        gacc[...] = jnp.zeros_like(gacc)
        sacc[...] = jnp.zeros_like(sacc)

        def block(n, _):
            r = pl.ds(al(n * 128, 128), 128)
            for cls in range(2):
                grp = group(u, cls)
                ln = pl.ds(cls * 128, 128)
                gain = gain_ref[pl.ds(grp, 1), :]
                shift = shift_ref[pl.ds(grp, 1), :]
                gated = gelu_value(vb[slot, r, ln].astype(F32))
                cen = gated - lane_mean(gated)
                inv = lax.rsqrt(lane_mean(cen * cen) + EPS)
                scaled = cen * inv
                gv_ref[0, r, cols(u, cls)] = scaled.astype(BF)
                sinv[u, r, ln] = jnp.broadcast_to(inv, (128, 128)).astype(BF)
                nb = (scaled * gain + shift).astype(BF)
                upper = gelu_value(ub[slot, r, ln].astype(F32))
                cot = gs[r, ln].astype(F32)
                dm = cot * upper
                dmb = dm.astype(BF)
                bacc[cls] += dm
                mixed = dot_nn(wl[grp], nb) + bb[cls]
                dn = dot_nn(wlt[grp], dmb)
                gwacc[cls] += dot_nt(dmb, nb)
                gt[pl.ds(cls * 128, 128), r] = (upper * mixed).T.astype(BF)
                gu_ref[0, r, cols(u, cls)] = (cot * mixed).astype(BF)
                prod = dn * scaled
                gacc[cls] += jnp.sum(prod.reshape(16, 8, 128), axis=0)
                sacc[cls] += jnp.sum(dn.reshape(16, 8, 128), axis=0)
                sdn[u, r, ln] = dn.astype(BF)
            return 0

        lax.fori_loop(0, 8, block, 0, unroll=4)

        @pl.when((u >= 1) & (u < 7))
        def _():
            arrive(u + 1)

        for lag, act in ((4, do_x), (3, do_s2a), (2, do_s1b), (1, do_ts)):

            @pl.when(u >= lag)
            def _(lag=lag, act=act):
                act(u - lag)

        pb[slot, :, :, pl.ds(0, WID)] = dot_nn(gt[...], d_v[...]).astype(BF).reshape(2, 128, WID)
        for cls in range(2):
            grp = group(u, cls)
            pb[slot, cls, :, pl.ds(WID, 128)] = jnp.where(tri, gwacc[cls], 0.0).astype(BF)
            st[0, pl.ds(grp, 1), :] = jnp.sum(bacc[cls].T, axis=0, keepdims=True)
            st[1, pl.ds(grp, 1), :] = jnp.sum(gacc[cls], axis=0, keepdims=True)
            st[2, pl.ds(grp, 1), :] = jnp.sum(sacc[cls], axis=0, keepdims=True)
        ps(u).start()

        return 0

    lax.fori_loop(0, 8, unit_body, 0)

    def v_copies(u):
        return uv_copies(u)

    def finish(u):
        slot = u % 2
        for cpy in v_copies(u):
            cpy.wait()
        if u < 7:
            for cpy in v_copies(u + 1):
                cpy.start()

        def block(n, _):
            r = pl.ds(al(n * 128, 128), 128)
            for cls in range(2):
                ln = pl.ds(cls * 128, 128)
                gain = gain_ref[pl.ds(group(u, cls), 1), :]
                cl = cols(u, cls)
                gu_ref[0, r, cl] = (
                    gu_ref[0, r, cl].astype(F32) * gelu_slope(ub[slot, r, ln].astype(F32))
                ).astype(BF)
                slope = gelu_slope(vb[slot, r, ln].astype(F32))
                scaled = gv_ref[0, r, cols(u, cls)].astype(F32)
                e = sdn[u, r, ln].astype(F32) * gain
                m1 = lane_mean(e)
                m2 = lane_mean(e * scaled)
                gv_ref[0, r, cols(u, cls)] = (
                    (e - m1 - scaled * m2) * (slope * sinv[u, r, ln].astype(F32))
                ).astype(BF)
            return 0

        lax.fori_loop(0, 8, block, 0, unroll=4)

    for cpy in v_copies(0):
        cpy.start()

    def stat_sum(src, parts, dst):
        acc = src[...]
        for part in parts:
            acc = acc + part[...]
        dst[...] = acc

    t0 = rdma(st, rs0, t_s.at[0, 0], t_r.at[0, 0], mate)
    t0.start()

    def tstage(k, d, src, f):
        return rdma(src, rs1.at[k, d - 1], t_s.at[k + 1, d - 1], t_r.at[k + 1, d - 1], f(d))

    def cz(d, j):
        return rdma(qc.at[pl.ds(2 * j, 2)], rc2.at[d - 1], c_s.at[1, d - 1], c_r.at[1, d - 1], pz(d))

    def cx(d):
        return rdma(qd, rc3.at[d - 1], c_s.at[2, d - 1], c_r.at[2, d - 1], px(d))

    def cgz(d, j):
        ref = cg.at[pl.ds(2 * j, 2), pl.ds(al(32 * y, 32), 32)]
        return rdma(ref, ref, c_s.at[3, d - 1], c_r.at[3, d - 1], pz(d))

    def cga(k, j):
        ref = cg.at[:, pl.ds(al(32 * j, 32), 32)]
        return rdma(ref, ref, c_s.at[4, k], c_r.at[4, k], py(HOP[k]))

    def cgb(k, j):
        ref = cg.at[pl.ds(4 * k, 4), pl.ds(al(32 * j, 32), 32)]
        return rdma(ref, ref, c_s.at[0, k], c_r.at[0, k], py(HOP[k]))


    def pipe(n):
        for lag, act in ((4, do_x), (3, do_s2a), (2, do_s1b), (1, do_ts)):
            if 0 <= n - lag <= 7:
                act(n - lag)

    def stat_step(k, f, g):
        for d in DS:
            tstage(k, d, st2.at[k], f).wait()
        if k < 2:
            stat_sum(st2.at[k], [rs1.at[k, i] for i in range(3)], st2.at[k + 1])
            for d in DS:
                tstage(k + 1, d, st2.at[k + 1], g).start()

    finish(0)
    pipe(8)
    t0.wait()
    stat_sum(st, [rs0], st2.at[0])
    for d in DS:
        tstage(0, d, st2.at[0], py).start()
    finish(1)
    pipe(9)
    for d in DS:
        cz(d, (z + d) % 4).start()
    stat_step(0, py, pz)
    finish(2)
    pipe(10)
    for d in DS:
        cz(d, (z + d) % 4).wait()
    acc = qc[pl.ds(2 * z, 2)].astype(F32)
    for k in range(3):
        acc = acc + rc2[k].astype(F32)
    qd[...] = acc.astype(BF)
    for d in DS:
        cx(d).start()
    stat_step(1, pz, px)
    finish(3)
    pipe(11)
    do_f(0)
    for d in DS:
        cx(d).wait()
    acc = qd[...].astype(F32)
    for k in range(3):
        acc = acc + rc3[k].astype(F32)
    cg[pl.ds(2 * z, 2), pl.ds(al(32 * y, 32), 32), :] = acc.astype(BF)
    for d in DS:
        cgz(d, z).start()
    stat_step(2, px, None)
    tot = st2[2]
    for k in range(3):
        tot = tot + rs1[2, k]
    stat_ref[...] = tot
    finish(4)
    do_f(1)
    do_g2a(0)
    for d in DS:
        cgz(d, (z + 4 - d) % 4).wait_recv()
    for k in range(2):
        cga(k, y).start()
    finish(5)
    do_g2a(1)
    do_g2b(0)
    for k in range(2):
        cga(k, (y + HOP[1 - k]) % 4).wait_recv()
    for k in range(2):
        cgb(k, (y + HOP[1 - k]) % 4).start()
    finish(6)
    do_g2b(1)
    for k in range(2):
        cgb(k, (y + 2) % 4).wait_recv()
    swap = rdma(cg, cp, c_s.at[5, 0], c_r.at[5, 0], mate)
    swap.start()
    finish(7)
    do_out(0)

    def gm_body(src, cls):
        def body(i, _):
            gm_ref[(i // 2) * 4 + 2 * cls + i % 2] = src[i].astype(F32)
            return 0

        lax.fori_loop(0, 8, body, 0)

    gm_body(cg, c)
    do_out(1)
    swap.wait()
    gm_body(cp, o)

    for k in range(6):
        wx(k).wait_send()
    for s in range(8):
        relay(s, c).wait_send()
    for u in range(2, 8):
        xs(u).wait_send()
    for g in range(2):
        for ab, d in PAIRS:
            g1(g, ab, d, i2[ab]).wait_send()
        for ab, k in BOTH:
            g2a(g, ab, k, i1[ab]).wait_send()
            g2b(g, ab, k, (i1[ab] + HOP[1 - k]) % 4).wait_send()
    for d in DS:
        cgz(d, z).wait_send()
    for k in range(2):
        cga(k, y).wait_send()
        cgb(k, (y + HOP[1 - k]) % 4).wait_send()


def place(gu, gv, gw, gm, st, o_gu, o_gv, o_gw, o_gm, o_b, o_g, o_s, sem):
    moves = [(gu, o_gu), (gv, o_gv), (gw, o_gw), (gm, o_gm), (st.at[0], o_b), (st.at[1], o_g), (st.at[2], o_s)]
    cps = [pltpu.make_async_copy(a, b, sem.at[i]) for i, (a, b) in enumerate(moves)]
    for cpy in cps:
        cpy.start()
    for cpy in cps:
        cpy.wait()


def on_device(u_pre, v_pre, d_out, w_mix, mix_bias, norm_gain, norm_shift, w_out):
    hbm = pl.BlockSpec(memory_space=pltpu.HBM)
    vm = pl.BlockSpec(memory_space=pltpu.VMEM)
    V = pltpu.VMEM
    DMA = pltpu.SemaphoreType.DMA
    scratch = [
        V((1024, WID), BF), V((8, 2, 128, WID), BF),
        V((2, 1024, 256), BF), V((2, 1024, 256), BF),
        V((1024, 256), BF), V((256, 1024), BF),
        V((2, 2, 128, EXT), BF), V((2, 128, EXT), BF), V((4, 128, WID), BF), V((4, 128, 128), BF),
        V((8, 2, 2, 16, 1024), BF), V((8, 2, 2, 32, 1024), BF), V((8, 3, 32, 128), BF), V((4, 2, 32, 1024), BF),
        V((8, 2, 3, 32, 256), BF),
        V((8, 2, 32, 256), BF), V((2, 4, 2, 32, 256), BF), V((256, WID), BF),
        V((8, 32, 128), BF), V((3, 2, 32, 128), BF),
        V((2, 32, 128), BF), V((3, 2, 32, 128), BF), V((8, 128, 128), BF), V((8, 128, 128), BF),
        V((3, 16, 128), F32), V((3, 3, 16, 128), F32), V((3, 16, 128), F32), V((3, 3, 3, 16, 128), F32),
        V((16, 128), F32), V((16, 128), F32), V((16, 128), F32),
        V((16, 128, 128), BF), V((16, 128, 128), BF), V((2, 128, 128), F32),
        V((2, 128, 128), F32), V((2, 128, 128), F32), V((2, 8, 128), F32), V((2, 8, 128), F32),
        V((8, 1024, 256), BF), V((8, 1024, 256), BF),
        DMA((10,)), DMA((2, 2, 2)), DMA((6,)), DMA((6,)), DMA((8,)), DMA((8,)),
        DMA((2,)), DMA((8,)), DMA((4, 2, 2, 2)), DMA((8, 2, 2, 2)), DMA((4, 2, 3)), DMA((8, 2, 3)),
        DMA((8,)), DMA((2, 4)), DMA((2, 2, 3)), DMA((2, 2, 3)), DMA((2, 2, 2, 2)), DMA((2, 2, 2, 2)),
        DMA((6, 3)), DMA((6, 3)), DMA((4, 3)), DMA((4, 3)), DMA((4, 3)), DMA((8, 3)),
    ]
    outs = pl.pallas_call(
        kernel,
        out_shape=(
            jax.ShapeDtypeStruct(u_pre.shape, BF),
            jax.ShapeDtypeStruct(v_pre.shape, BF),
            jax.ShapeDtypeStruct((256, WID), F32),
            jax.ShapeDtypeStruct((16, 128, 128), F32),
            jax.ShapeDtypeStruct((3, 16, 128), F32),
        ),
        in_specs=[hbm] * 8,
        out_specs=(vm, vm, vm, vm, vm),
        scratch_shapes=scratch,
        compiler_params=pltpu.CompilerParams(
            collective_id=0, has_side_effects=True, vmem_limit_bytes=39 * 1024 * 1024
        ),
    )(u_pre, v_pre, d_out, w_mix, mix_bias, norm_gain, norm_shift, w_out)
    anyspace = pl.BlockSpec(memory_space=pl.ANY)
    small = jax.ShapeDtypeStruct((16, 128), F32)
    return pl.pallas_call(
        place,
        out_shape=(
            jax.ShapeDtypeStruct(u_pre.shape, BF),
            jax.ShapeDtypeStruct(v_pre.shape, BF),
            jax.ShapeDtypeStruct((256, WID), F32),
            jax.ShapeDtypeStruct((16, 128, 128), F32),
            small, small, small,
        ),
        in_specs=[anyspace] * 5,
        out_specs=(hbm,) * 7,
        scratch_shapes=[DMA((7,))],
        compiler_params=pltpu.CompilerParams(vmem_limit_bytes=512 * 1024),
    )(*outs)


def solution(mesh):
    return jax.shard_map(
        on_device,
        mesh=mesh,
        in_specs=(
            P("dp", "sp", None), P("dp", "sp", None), P("dp", "sp", None),
            P(), P(), P(), P(), P("dp", None),
        ),
        out_specs=(P("dp", "sp", None), P("dp", "sp", None), P("dp", None), P(), P(), P(), P()),
        check_vma=False,
    )
```
